128 devices in a mesh: ep: 32 (over z, y, core), tp: 4 (over x).
Axes of the slice: x: 4, y: 4, z: 4, core: 2. Of those that a mesh axis runs over, the one named last changes fastest.
Arguments:
- mixer_input_rows: bfloat16 [16384, 2048], P(('ep', 'tp')), may hold values from -6 to 6
- mixer_norm_scale: float32 [2048], replicated, may hold values from 0.1 to 1.9
- decay_bias_table: float32 [16384, 16], P('ep', 'tp'), may hold values from -14 to 1
- erase_bias_table: float32 [16], P('tp'), may hold values from -12 to 1
- receive_weight: bfloat16 [2048, 1024], P(None, 'tp'), may hold values from -0.125 to 0.125
- key_weight: bfloat16 [2048, 1024], P(None, 'tp'), may hold values from -0.125 to 0.125
- value_weight: bfloat16 [2048, 1024], P(None, 'tp'), may hold values from -0.125 to 0.125
- decay_weight: bfloat16 [2048, 1024], P(None, 'tp'), may hold values from -0.125 to 0.125
- erase_weight: bfloat16 [2048, 1024], P(None, 'tp'), may hold values from -0.125 to 0.125
- self_token_scale: float32 [16, 64], P('tp'), may hold values from -0.6 to 0.6
- head_norm_scale: float32 [1024], P('tp'), may hold values from 0.1 to 1.9
- output_weight: bfloat16 [1024, 2048], P('tp'), may hold values from -0.1875 to 0.1875
- expert_input_rows: bfloat16 [16384, 2048], P(('ep', 'tp')), may hold values from -6 to 6
- expert_norm_scale: float32 [2048], replicated, may hold values from 0.1 to 1.9
- routes: int32 [16384, 2], P(('ep', 'tp')), may hold values from 0 to 127, all different within a row; in each aligned block of 128 rows (0 to 127, 128 to 255, ...) at most 4 rows name the same one
- router_weights: float32 [16384, 2], P(('ep', 'tp')), may hold values from 0.1 to 1
- routed_gate_weight: bfloat16 [128, 2048, 1024], P(('ep', 'tp')), may hold values from -0.125 to 0.125
- routed_up_weight: bfloat16 [128, 2048, 1024], P(('ep', 'tp')), may hold values from -0.125 to 0.125
- routed_down_weight: bfloat16 [128, 1024, 2048], P(('ep', 'tp')), may hold values from -0.1875 to 0.1875
- common_gate_weight: bfloat16 [2048, 256], replicated, may hold values from -0.125 to 0.125
- common_up_weight: bfloat16 [2048, 256], replicated, may hold values from -0.125 to 0.125
- common_down_weight: bfloat16 [256, 2048], replicated, may hold values from -0.375 to 0.375
Outputs:
- mixer_output: bfloat16 [16384, 2048], P(('ep', 'tp'))
- mixed_b: bfloat16 [16384, 2048], P(('ep', 'tp'))
The draws below stay inside these ranges and needn't reach their ends.
Inputs may be any that keep to these rules, and one draw needn't show every extreme that they name: `routes`: within the rows of one device no expert is named by more than 4 rows, a bound that some block reaches; each row names 2 different experts, and every expert is named somewhere.
All inputs are finite; a program needn't handle non-finite values.
Results may differ from the reference program's by a relative error of at most 0.015.
Values may be sent and summed in bfloat16 or wider, within the bound.
A program may use at most 128 MiB of HBM per device.

```python
import math
import jax
import jax.numpy as jnp
import numpy as np
from jax import lax

D = 2048
MIXER_HEADS = 16
HEAD_CHANNELS = 64
MIX = 1024
EXPERT_FF = 1024
SHARED_FF = 256
TOPK = 2
TOK_DEV = 128
SEQ_DEV = 512
BATCH_TOKENS = 16384
EXPERTS = 128
CAP = 4
N_TP = 4


def head_speeds(key):
    shuffled = jax.random.permutation(jax.random.fold_in(key, 4101), MIXER_HEADS)
    fast_count = MIXER_HEADS // 2
    return shuffled < fast_count


def draw_mixer_input_rows(key, part):
    block_total = BATCH_TOKENS // 64
    order_key, direction_key, noise_key = jax.random.split(jax.random.fold_in(key, 4104), 3)
    picked = jax.random.permutation(order_key, block_total) < max(block_total // 8, 1)
    directions = jax.random.normal(direction_key, (block_total, D), jnp.float32)
    noise = jax.random.normal(noise_key, (BATCH_TOKENS, D), jnp.float32)
    aligned_rows = jnp.repeat(picked, 64)
    shared_rows = jnp.repeat(directions, 64, axis=0)
    rows = jnp.where(aligned_rows[:, None], 2.4 * shared_rows + 0.6 * noise, noise)
    return jnp.clip(rows, -6.0, 6.0).astype(jnp.bfloat16)


def draw_decay_bias_table(key, part):
    fast_heads = head_speeds(key)
    tier_random_key, spike_key, head_random_key = jax.random.split(jax.random.fold_in(key, 4102), 3)
    block_level = jax.random.uniform(tier_random_key, (BATCH_TOKENS // SEQ_DEV,), jnp.float32, -0.7, 0.7)
    gradual_tier = jnp.log(0.5 / BATCH_TOKENS) + jnp.repeat(block_level, SEQ_DEV)
    token_position = jnp.arange(BATCH_TOKENS, dtype=jnp.int32)
    spike_groups = jax.random.randint(spike_key, (3,), 0, BATCH_TOKENS)
    spike_rows = jnp.any(token_position[:, None] == spike_groups[None, :], axis=1)
    gradual_rows = jnp.where(spike_rows, 0.4, gradual_tier)
    fast_level = jnp.log(0.02) + 0.5 + jax.random.uniform(head_random_key, (MIXER_HEADS,), jnp.float32, -0.4, 0.4)
    return jnp.where(fast_heads[None, :], fast_level[None, :], gradual_rows[:, None]).astype(jnp.float32)


def draw_erase_bias_table(key, part):
    fast_heads = head_speeds(key)
    spread = jax.random.uniform(jax.random.fold_in(key, 4103), (MIXER_HEADS,), jnp.float32, -0.5, 0.5)
    return jnp.where(fast_heads, 0.75 + 0.5 * spread, jnp.log(16.0 / BATCH_TOKENS) + spread).astype(jnp.float32)


def steps_of(key, extent, shards, least, top_value):
    factor_of, own = 1.0, jax.random.fold_in(key, 6)
    for position, shards_of in shards:
        draws = jnp.exp(jax.random.uniform(jax.random.fold_in(own, position), (shards_of,), jnp.float32, least / len(shards), top_value / len(shards)))
        factor_of = factor_of * jnp.repeat(draws, extent[position] // shards_of).reshape([-1 if axis == position else 1 for axis in range(len(extent))])
    return factor_of


def assign_block(rng, own, number, rows, amount, top, most, lean):
    ranking = jax.random.permutation(rng, amount)
    heavy_load, usual = load_shares(amount, rows * top, most, lean, True), load_shares(amount, rows * top, most, lean, False)
    places = jnp.arange(amount)

    def named(sizes, turn):
        used = int((sizes > 0).sum())
        fixed = max(1, used // 4)
        moved = fixed + (places - fixed + turn * (used - fixed)) % max(1, amount - fixed)
        return jnp.zeros((amount,), jnp.int32).at[ranking[jnp.where(places < fixed, places, moved)]].set(jnp.asarray(sizes, jnp.int32))

    sizes = jnp.where(number % 4 == 0, named(heavy_load, number // 4), named(usual, number - number // 4 - 1))
    mixed = jax.random.permutation(jax.random.fold_in(own, 3), amount)
    source_of, receiver = mixed[0:amount // 2 * 2:2], mixed[1:amount // 2 * 2:2]
    room = jnp.minimum(sizes[source_of] - 1, most - sizes[receiver]) // 2
    room = jnp.where((source_of == ranking[0]) | (receiver == ranking[0]) | (sizes[receiver] == 0), 0, jnp.maximum(room, 0))
    moved = jax.random.randint(jax.random.fold_in(own, 4), (amount // 2,), 0, 1 << 20) % (room + 1)
    sizes = sizes.at[source_of].add(-moved).at[receiver].add(moved)
    labels = jnp.searchsorted(jnp.cumsum(sizes), jnp.arange(rows * top), side="right").astype(jnp.int32)
    listing = labels.reshape(top, rows).T
    listing = listing[jax.random.permutation(jax.random.fold_in(own, 1), rows)]
    turn = jax.random.randint(jax.random.fold_in(own, 2), (rows, 1), 0, top)
    return jnp.take_along_axis(listing, (jnp.arange(top)[None, :] + turn) % top, axis=1)


def load_shares(amount, total, bound, lean, full):
    portions = [(1 << 20) // math.isqrt(standing ** lean) + 1 for standing in range(1, amount + 1)]
    largest = bound if full else min(bound, max(-(-total // amount), total * portions[0] // sum(portions)))
    least = 1 if total - largest >= amount - 1 else 0
    counts, rest = [largest] + [least] * (amount - 1), total - largest - least * (amount - 1)
    while rest > 0:
        free = [i for i in range(1, amount) if counts[i] < largest] or [i for i in range(1, amount) if counts[i] < bound]
        mass, remaining = sum([portions[i] for i in free]), rest
        for i in free:
            addition = min(bound - counts[i], max(1, remaining * portions[i] // mass), rest)
            counts[i] = counts[i] + addition
            rest = rest - addition
    return np.array(counts)


def scatter_about(stream_key, extent, scale, limit, pieces=(), kind=jnp.bfloat16):
    values = scale * jax.random.normal(stream_key, extent, jnp.float32)
    if pieces:
        values = values * steps_of(stream_key, extent, pieces, -0.22, 0.18)
    return jnp.clip(values, -limit, limit).astype(kind)


def setup_inputs(seed: int = 0) -> dict:
    key_of = jax.random.split(jax.random.key(seed), 23)
    mixer_input_rows = draw_mixer_input_rows(jax.random.fold_in(key_of[22], 71), 0)
    mixer_norm_scale = jnp.clip(1.0 + 0.18 * jax.random.normal(key_of[1], (D,), jnp.float32), 0.1, 1.9)
    decay_bias_table = draw_decay_bias_table(jax.random.fold_in(key_of[22], 71), 0)
    erase_bias_table = draw_erase_bias_table(jax.random.fold_in(key_of[22], 71), 0)
    receive_weight = scatter_about(key_of[4], (D, MIX), D ** -0.5, 0.125, ((1, 4),))
    key_weight = scatter_about(key_of[5], (D, MIX), D ** -0.5, 0.125, ((1, 4),))
    value_weight = scatter_about(key_of[6], (D, MIX), D ** -0.5, 0.125, ((1, 4),))
    decay_weight = scatter_about(key_of[7], (D, MIX), D ** -0.5, 0.125, ((1, 4),))
    erase_weight = scatter_about(key_of[8], (D, MIX), D ** -0.5, 0.125, ((1, 4),))
    self_token_scale = scatter_about(key_of[9], (MIXER_HEADS, HEAD_CHANNELS), 0.1, 0.6, ((0, 4),), jnp.float32)
    head_norm_scale = jnp.clip(1.0 + 0.18 * jax.random.normal(key_of[10], (MIX,), jnp.float32), 0.1, 1.9)
    output_weight = scatter_about(key_of[11], (MIX, D), MIX ** -0.5, 0.1875, ((0, 4),))
    expert_input_rows = scatter_about(key_of[12], (BATCH_TOKENS, D), 1.0, 6.0, ((0, 128),))
    expert_norm_scale = jnp.clip(1.0 + 0.18 * jax.random.normal(key_of[13], (D,), jnp.float32), 0.1, 1.9)
    routes_keys = jax.random.split(jax.random.fold_in(key_of[14], 1), BATCH_TOKENS // TOK_DEV)
    routes_turns = jax.random.permutation(jax.random.fold_in(key_of[14], 3), BATCH_TOKENS // TOK_DEV)
    routes = jax.vmap(lambda own, number: assign_block(jax.random.fold_in(key_of[14], 2), own, number, TOK_DEV, EXPERTS, TOPK, CAP, 1))(routes_keys, routes_turns).reshape((BATCH_TOKENS, TOPK))
    router_weights = jnp.clip(jnp.exp(math.log(1.0) - 2.3025851 * jax.random.uniform(key_of[15], (BATCH_TOKENS, TOPK), jnp.float32) ** steps_of(key_of[15], (BATCH_TOKENS, TOPK), ((0, 128),), -0.2, 0.2)), 0.1, 1.0)
    routed_gate_weight = scatter_about(key_of[16], (EXPERTS, D, EXPERT_FF), D ** -0.5, 0.125, ((0, 128),))
    routed_up_weight = scatter_about(key_of[17], (EXPERTS, D, EXPERT_FF), D ** -0.5, 0.125, ((0, 128),))
    routed_down_weight = scatter_about(key_of[18], (EXPERTS, EXPERT_FF, D), EXPERT_FF ** -0.5, 0.1875, ((0, 128),))
    common_gate_weight = scatter_about(key_of[19], (D, SHARED_FF), D ** -0.5, 0.125)
    common_up_weight = scatter_about(key_of[20], (D, SHARED_FF), D ** -0.5, 0.125)
    common_down_weight = scatter_about(key_of[21], (SHARED_FF, D), SHARED_FF ** -0.5, 0.375)
    return dict(mixer_input_rows=mixer_input_rows, mixer_norm_scale=mixer_norm_scale, decay_bias_table=decay_bias_table, erase_bias_table=erase_bias_table, receive_weight=receive_weight, key_weight=key_weight, value_weight=value_weight, decay_weight=decay_weight, erase_weight=erase_weight, self_token_scale=self_token_scale, head_norm_scale=head_norm_scale, output_weight=output_weight, expert_input_rows=expert_input_rows, expert_norm_scale=expert_norm_scale, routes=routes, router_weights=router_weights, routed_gate_weight=routed_gate_weight, routed_up_weight=routed_up_weight, routed_down_weight=routed_down_weight, common_gate_weight=common_gate_weight, common_up_weight=common_up_weight, common_down_weight=common_down_weight)


precise = lax.Precision.HIGHEST

def rms_rows(values, feature_gain):
    wide_values = values.astype(jnp.float32)
    inverse = lax.rsqrt(lax.optimization_barrier(jnp.mean(wide_values * wide_values, axis=-1, keepdims=True)) + 1e-06)
    return (wide_values * inverse * feature_gain).astype(jnp.bfloat16)

def mixer_baseline(mixer_input_rows, mixer_norm_scale, decay_bias_table, erase_bias_table, receive_weight, key_weight, value_weight, decay_weight, erase_weight, self_token_scale, head_norm_scale, output_weight):
    normed_a = rms_rows(mixer_input_rows, mixer_norm_scale)
    token_count = normed_a.shape[0]

    def heads_of(weight_part):
        product = jnp.dot(normed_a, weight_part, preferred_element_type=jnp.float32)
        return product.reshape(token_count, MIXER_HEADS, HEAD_CHANNELS)
    receive_vector = heads_of(receive_weight)
    key_projected = heads_of(key_weight)
    value_projected = heads_of(value_weight)
    log_decay = -jnp.exp(-jax.nn.softplus(-(heads_of(decay_weight) + decay_bias_table[:, :, None])) - 0.5)
    erase_rate = jax.nn.sigmoid(heads_of(erase_weight) + erase_bias_table[None, :, None])
    unit_key = key_projected * lax.rsqrt(lax.optimization_barrier(jnp.sum(key_projected * key_projected, axis=2, keepdims=True)) + 1e-06)

    def advance(state_now, inputs):
        receptance_now, decay_now, key_now, value_now, unit_now, rate_now = inputs
        projected = jnp.einsum('hvk,hk->hv', state_now, unit_now, precision=precise)
        state_now = state_now * jnp.exp(decay_now)[:, None, :] - projected[:, :, None] * (unit_now * rate_now)[:, None, :] + value_now[:, :, None] * key_now[:, None, :]
        return (state_now, jnp.einsum('hvk,hk->hv', state_now, receptance_now, precision=precise))
    start_state = jnp.zeros((MIXER_HEADS, HEAD_CHANNELS, HEAD_CHANNELS), jnp.float32)
    readout = lax.scan(advance, start_state, (receive_vector, log_decay, key_projected, value_projected, unit_key, erase_rate))[1]
    mean_removed = readout - lax.optimization_barrier(jnp.mean(readout, axis=2, keepdims=True))
    squared_mean = lax.optimization_barrier(jnp.mean(mean_removed * mean_removed, axis=2, keepdims=True))
    head_norm_scales = head_norm_scale.reshape(MIXER_HEADS, HEAD_CHANNELS)
    self_token_term = lax.optimization_barrier(jnp.sum(receive_vector * key_projected * self_token_scale[None], axis=2, keepdims=True)) * value_projected
    mixer_head_count = mean_removed * lax.rsqrt(squared_mean + 0.00064) * head_norm_scales + self_token_term
    mixer_head_count = mixer_head_count.reshape(token_count, MIXER_HEADS * HEAD_CHANNELS).astype(jnp.bfloat16)
    group_width = MIXER_HEADS * HEAD_CHANNELS // N_TP
    summed_total = jnp.zeros((token_count, D), jnp.float32)
    for group_index in range(N_TP):
        first_column = group_index * group_width
        partial_sum = jnp.dot(mixer_head_count[:, first_column:first_column + group_width], output_weight[first_column:first_column + group_width], preferred_element_type=jnp.float32).astype(jnp.bfloat16)
        summed_total = summed_total + lax.optimization_barrier(partial_sum).astype(jnp.float32)
    return summed_total.astype(jnp.bfloat16)

def experts_reference(expert_input_rows, expert_norm_scale, routes, router_weights, routed_gate_weight, routed_up_weight, routed_down_weight, common_gate_weight, common_up_weight, common_down_weight):
    normed_b = rms_rows(expert_input_rows, expert_norm_scale)
    route_weight = 2.5 * router_weights / lax.optimization_barrier(jnp.sum(router_weights, axis=1, keepdims=True))
    block_count = BATCH_TOKENS // TOK_DEV
    pair_count = TOK_DEV * TOPK
    chosen = routes.reshape(block_count, pair_count)
    onehot = (chosen[:, :, None] == jnp.arange(EXPERTS, dtype=jnp.int32)[None, None, :]).astype(jnp.int32)
    slot_rank = lax.optimization_barrier(jnp.sum(jnp.cumsum(onehot, axis=1) * onehot, axis=2)) - 1
    slot_index = chosen * CAP + slot_rank
    block_index = jnp.arange(block_count, dtype=jnp.int32)[:, None]
    global_row = block_index * TOK_DEV + (jnp.arange(pair_count, dtype=jnp.int32) // TOPK)[None, :]
    token_table = jnp.zeros((block_count, EXPERTS * CAP), jnp.int32).at[block_index, slot_index].set(global_row)
    weight_table = jnp.zeros((block_count, EXPERTS * CAP), jnp.float32).at[block_index, slot_index].set(route_weight.reshape(block_count, pair_count))
    token_table = token_table.reshape(block_count, EXPERTS, CAP).transpose(1, 0, 2).reshape(EXPERTS, -1)
    weight_table = weight_table.reshape(block_count, EXPERTS, CAP).transpose(1, 0, 2).reshape(EXPERTS, -1)

    def one_expert(running, expert_inputs):
        gate_part, up_part, down_part, token_index, weight_part = expert_inputs
        expert_rows = normed_b[token_index]
        expert_hidden = (jax.nn.silu(jnp.dot(expert_rows, gate_part, preferred_element_type=jnp.float32)) * jnp.dot(expert_rows, up_part, preferred_element_type=jnp.float32)).astype(jnp.bfloat16)
        expert_out = jnp.dot(expert_hidden, down_part, preferred_element_type=jnp.float32).astype(jnp.bfloat16)
        running = running.at[token_index].add(weight_part[:, None] * expert_out.astype(jnp.float32))
        return (running, None)
    routed = lax.scan(one_expert, jnp.zeros((BATCH_TOKENS, D), jnp.float32), (routed_gate_weight, routed_up_weight, routed_down_weight, token_table, weight_table))[0]
    shared_hidden = (jax.nn.silu(jnp.dot(normed_b, common_gate_weight, preferred_element_type=jnp.float32)) * jnp.dot(normed_b, common_up_weight, preferred_element_type=jnp.float32)).astype(jnp.bfloat16)
    shared_term = jnp.dot(shared_hidden, common_down_weight, preferred_element_type=jnp.float32)
    return (routed + shared_term).astype(jnp.bfloat16)

def reference(mixer_input_rows, mixer_norm_scale, decay_bias_table, erase_bias_table, receive_weight, key_weight, value_weight, decay_weight, erase_weight, self_token_scale, head_norm_scale, output_weight, expert_input_rows, expert_norm_scale, routes, router_weights, routed_gate_weight, routed_up_weight, routed_down_weight, common_gate_weight, common_up_weight, common_down_weight):
    mixer_output = mixer_baseline(mixer_input_rows, mixer_norm_scale, decay_bias_table, erase_bias_table, receive_weight, key_weight, value_weight, decay_weight, erase_weight, self_token_scale, head_norm_scale, output_weight)
    mixed_b = experts_reference(expert_input_rows, expert_norm_scale, routes, router_weights, routed_gate_weight, routed_up_weight, routed_down_weight, common_gate_weight, common_up_weight, common_down_weight)
    return (mixer_output, mixed_b)
```

```python
import functools

import jax
import jax.numpy as jnp
from jax import lax
from jax.experimental import pallas as pl
from jax.experimental.pallas import tpu as pltpu
from jax.sharding import Mesh
from jax.sharding import PartitionSpec as P

EP = ("ep_0", "ep_1", "ep_2")
EP_TP = ("ep_0", "ep_1", "ep_2", "tp")
MESH = pl.DeviceIdType.MESH
BF = jnp.bfloat16
F32 = jnp.float32
VMEM = pltpu.VMEM
CHUNK = 64
PAIR = 128


def mm(a, b):
    return lax.dot_general(a, b, (((1,), (0,)), ((), ())), preferred_element_type=F32)


def mm_t(a, b):
    return lax.dot_general(a, b, (((1,), (1,)), ((), ())), preferred_element_type=F32)


def mm_tn(a, b):
    return lax.dot_general(a, b, (((0,), (0,)), ((), ())), preferred_element_type=F32)


def split2(x):
    hi = x.astype(BF)
    lo = (x - hi.astype(F32)).astype(BF)
    return hi, lo


def iota(shape, dim):
    return lax.broadcasted_iota(jnp.int32, shape, dim)


def pair_mask():
    return (iota((PAIR, PAIR), 0) // 64) == (iota((PAIR, PAIR), 1) // 64)


def block_diag(x, mask):
    return jnp.concatenate([x, x], axis=0) * mask


def head_sums(x, mask):
    hi, lo = split2(x)
    return mm(hi, mask) + mm(lo, mask)


def mixer_kernel(
    rows_ref, wr_ref, wk_ref, wv_ref, wd_ref, we_ref, db_ref, eb_ref, st_ref,
    out_ref, rt_ref, self_ref, tl_ref,
    pr_ref, r_s, e_s, l_s, d_s,
):
    n_rows = rows_ref.shape[0]
    n_chunks = n_rows // CHUNK
    group = 4
    mask_b = pair_mask()
    mask = mask_b.astype(F32).astype(BF)
    for j, w in enumerate((wr_ref, wk_ref, wv_ref, wd_ref, we_ref)):
        pr_ref[:, j * 256 : (j + 1) * 256] = mm(rows_ref[...], w[...])

    t_i = iota((CHUNK, PAIR), 0)
    s_i = iota((CHUNK, PAIR), 1) % 64
    strict = t_i > s_i
    causal = t_i >= s_i
    eye = (t_i == s_i).astype(F32)
    lane_lo = iota((CHUNK, PAIR), 1) < 64
    tril = (iota((CHUNK, CHUNK), 0) >= iota((CHUNK, CHUNK), 1)).astype(F32).astype(BF)

    def do_group(g, carry):
        units = []
        for cc in range(group):
            for p in range(2):
                r0 = pl.multiple_of((g * group + cc) * CHUNK, CHUNK)
                rows = pl.ds(r0, CHUNK)
                lanes = slice(p * PAIR, (p + 1) * PAIR)
                col = lambda j: pr_ref[rows, j * 256 + p * PAIR : j * 256 + (p + 1) * PAIR]
                r, k, v, dp, ep = (col(j) for j in range(5))
                db = db_ref[rows, :]
                db = jnp.where(lane_lo, db[:, 2 * p : 2 * p + 1], db[:, 2 * p + 1 : 2 * p + 2])
                ld = -0.6065306597126334 / (1.0 + jnp.exp(-(dp + db)))
                er = 1.0 / (1.0 + jnp.exp(-(ep + eb_ref[:, lanes])))
                u = k * lax.rsqrt(head_sums(k * k, mask) + 1e-06)
                self_ref[rows, lanes] = head_sums(r * k * st_ref[:, lanes], mask) * v
                hi, lo = split2(ld)
                cum = mm(tril, hi) + mm(tril, lo)
                end = cum[CHUNK - 1 : CHUNK, :]
                eci = jnp.exp(-cum)
                a = (-u * jnp.exp(cum - ld)).astype(BF)
                ri = r * jnp.exp(cum)
                ue = u * er
                b = (ue * eci).astype(BF)
                ko = (k * eci).astype(BF)
                tail = jnp.exp(end - cum)
                bt = (ue * tail).astype(BF)
                kt = (k * tail).astype(BF)
                ar = jnp.concatenate([a, ri.astype(BF)], axis=0)
                m13 = mm_t(ar, block_diag(b, mask))
                m24 = mm_t(ar, block_diag(ko, mask))
                m1 = jnp.where(strict, m13[:CHUNK], 0.0)
                m3 = jnp.where(causal, m13[CHUNK:], 0.0).astype(BF)
                m24 = jnp.concatenate(
                    [jnp.where(strict, m24[:CHUNK], 0.0), jnp.where(causal, m24[CHUNK:], 0.0)], axis=0
                ).astype(BF)
                vb = v.astype(BF)
                mv = mm(m24, block_diag(vb, mask))
                x = eye + jnp.where((t_i // 2) == (s_i // 2), m1, 0.0)
                units.append(
                    dict(rows=rows, lanes=lanes, p=p, r0=r0, a=a, ri=ri, m1=m1, m3=m3, mv=mv, x=x,
                         bt=bt, kt=kt, vb=vb, end=end)
                )
        size = 2
        while size < CHUNK:
            corner = ((t_i // (2 * size)) == (s_i // (2 * size))) & ((t_i // size) != (s_i // size))
            for n in units:
                xb = n["x"].astype(BF)
                n["xb"] = xb
                c = jnp.where(corner, n["m1"], 0.0).astype(BF)
                n["y"] = mm(xb, block_diag(c, mask)).astype(BF)
            for n in units:
                n["x"] = n["x"] + mm(n["y"], block_diag(n["xb"], mask))
            size *= 2
        for n in units:
            right = jnp.concatenate(
                [block_diag(n["a"], mask), block_diag(n["mv"][:CHUNK].astype(BF), mask)], axis=1
            )
            n["pq"] = mm(n["x"].astype(BF), right).astype(BF)
        for n in units:
            pb, qb = n["pq"][:, :PAIR], n["pq"][:, PAIR:]
            m3pq = mm(n["m3"], jnp.concatenate([block_diag(pb, mask), block_diag(qb, mask)], axis=1))
            r_s[n["rows"], n["lanes"]] = (n["ri"] + m3pq[:, :PAIR]).astype(BF)
            out_ref[n["rows"], n["lanes"]] = m3pq[:, PAIR:] + n["mv"][CHUNK:]
            big = pl.ds(pl.multiple_of(n["r0"] * 2, PAIR), PAIR)
            e_s[big, n["lanes"]] = (mm_tn(pb, n["bt"]) * mask).astype(BF)
            left = jnp.concatenate([qb, n["vb"]], axis=0)
            right = jnp.concatenate([n["bt"], n["kt"]], axis=0)
            l_s[big, n["lanes"]] = mm_tn(left, right) * mask
            small = pl.ds(pl.multiple_of(n["r0"] // 8, 8), 8)
            d_s[small, n["lanes"]] = jnp.broadcast_to(jnp.exp(n["end"]), (8, PAIR))
        return carry

    lax.fori_loop(0, n_chunks // group, do_group, 0)

    eye2 = (iota((PAIR, PAIR), 0) == iota((PAIR, PAIR), 1)).astype(F32)
    state = [jnp.concatenate([jnp.zeros((PAIR, PAIR), F32), eye2], axis=0) for _ in range(2)]
    for c in range(n_chunks):
        rows = slice(c * CHUNK, (c + 1) * CHUNK)
        big = slice(c * PAIR, (c + 1) * PAIR)
        for p in range(2):
            lanes = slice(p * PAIR, (p + 1) * PAIR)
            sb = state[p].astype(BF)
            o = mm_t(r_s[rows, lanes], sb)
            out_ref[rows, lanes] = out_ref[rows, lanes] + o[:, :PAIR]
            rt_ref[rows, lanes] = o[:, PAIR:].astype(BF)
            decayed = state[p] * d_s[c * 8 : c * 8 + 1, lanes]
            moved = mm(sb, e_s[big, lanes])
            state[p] = decayed + moved
            state[p] = jnp.concatenate([state[p][:PAIR] + l_s[big, lanes], state[p][PAIR:]], axis=0)
    for p in range(2):
        lanes = slice(p * PAIR, (p + 1) * PAIR)
        tl_ref[0:64, lanes] = (state[p][PAIR : PAIR + 64] + state[p][PAIR + 64 :]).astype(BF)
        tl_ref[64:128, lanes] = (state[p][0:64] + state[p][64:128]).astype(BF)


def state_kernel(tl_ref, enter_ref, cbuf, ysend, ybuf, zsend, zbuf, cs, cr, ys, yr, zs, zr):
    z, y, c = lax.axis_index("ep_0"), lax.axis_index("ep_1"), lax.axis_index("ep_2")
    barrier = pltpu.get_barrier_semaphore()
    pl.semaphore_signal(barrier, inc=1, device_id={"ep_2": 1 - c}, device_id_type=MESH)
    for d in range(1, 4):
        pl.semaphore_signal(barrier, inc=1, device_id={"ep_1": (y + d) % 4}, device_id_type=MESH)
        pl.semaphore_signal(barrier, inc=1, device_id={"ep_0": (z + d) % 4}, device_id_type=MESH)
    pl.semaphore_wait(barrier, 7)
    mask = pair_mask().astype(F32).astype(BF)

    def times(left, t):
        return jnp.concatenate(
            [mm(left[:, q * PAIR : (q + 1) * PAIR].astype(BF),
                block_diag(t[:, q * PAIR : (q + 1) * PAIR].astype(BF), mask)) for q in range(2)],
            axis=1,
        )

    def compose(early, late):
        joined = times(early, late[:64])
        return jnp.concatenate([joined[:64], joined[64:] + late[64:]], axis=0)

    cp = pltpu.make_async_remote_copy(
        src_ref=tl_ref, dst_ref=cbuf, send_sem=cs, recv_sem=cr,
        device_id={"ep_2": 1 - c}, device_id_type=MESH)
    cp.start()
    cp.wait()
    mine = tl_ref[...].astype(F32)
    other = cbuf[...].astype(F32)
    first = jnp.where(c == 0, mine, other)
    second = jnp.where(c == 0, other, mine)

    def exchange(value, send, buf, ss, rs, axis, me):
        send[...] = value.astype(BF)
        copies = []
        for d in range(1, 4):
            cp = pltpu.make_async_remote_copy(
                src_ref=send, dst_ref=buf.at[d], send_sem=ss.at[d], recv_sem=rs.at[d],
                device_id={axis: (me + d) % 4}, device_id_type=MESH)
            cp.start()
            copies.append(cp)
        buf[0] = value.astype(BF)
        for cp in copies:
            cp.wait()

    exchange(compose(first, second), ysend, ybuf, ys, yr, "ep_1", y)
    run = ybuf[y % 4].astype(F32)
    ident = (iota((64, 256), 0) == iota((64, 256), 1) % 64).astype(F32)
    before = jnp.concatenate([ident, jnp.zeros((64, 256), F32)], axis=0)
    for j in range(1, 4):
        before = jnp.where(y == j, run, before)
        run = compose(run, ybuf[(y - j + 4) % 4].astype(F32))
    exchange(run, zsend, zbuf, zs, zr, "ep_0", z)
    state = jnp.zeros((64, 256), F32)
    enter = state
    for j in range(0, 3):
        piece = zbuf[(z - j + 4) % 4].astype(F32)
        state = (times(state, piece[:64]) if j else 0.0) + piece[64:]
        enter = jnp.where(z == j + 1, state, enter)
    enter = times(enter, before[:64]) + before[64:]
    enter = jnp.where(c == 0, enter, times(enter, first[:64]) + first[64:])
    enter_ref[...] = enter.astype(BF)


def finish_kernel(out_ref, rt_ref, self_ref, enter_ref, gain_ref, w_ref, part_ref, heads):
    mask = pair_mask().astype(F32).astype(BF)
    for p in range(2):
        lanes = slice(p * PAIR, (p + 1) * PAIR)
        ent = block_diag(enter_ref[:, lanes], mask)
        o = out_ref[:, lanes] + mm_t(rt_ref[:, lanes], ent)
        o = o - head_sums(o, mask) * (1.0 / 64)
        var = head_sums(o * o, mask) * (1.0 / 64)
        h = o * lax.rsqrt(var + 0.00064) * gain_ref[:, lanes] + self_ref[:, lanes]
        heads[:, lanes] = h.astype(BF)
    for j in range(4):
        cols = slice(j * 512, (j + 1) * 512)
        part_ref[:, cols] = mm(heads[...], w_ref[:, cols]).astype(BF)


def vspec(n):
    return [pl.BlockSpec(memory_space=VMEM)] * n


def copy_for_each(value, axis):
    copies = jnp.broadcast_to(value, (lax.axis_size(axis), *value.shape))
    return lax.all_to_all(copies, axis, split_axis=0, concat_axis=0, tiled=True)


def rms_rows(values, feature_gain):
    wide_values = values.astype(F32)
    inverse = lax.rsqrt(jnp.mean(wide_values * wide_values, axis=1, keepdims=True) + 1e-06)
    return (wide_values * inverse * feature_gain).astype(BF)


def per_device(
    mixer_input_rows, mixer_norm_scale, decay_bias_table, erase_bias_table,
    receive_weight, key_weight, value_weight, decay_weight, erase_weight,
    self_token_scale, head_norm_scale, output_weight,
    expert_input_rows, expert_norm_scale, routes, router_weights,
    routed_gate_weight, routed_up_weight, routed_down_weight,
    common_gate_weight, common_up_weight, common_down_weight,
):
    normed_a = rms_rows(mixer_input_rows, mixer_norm_scale)
    row_piece = copy_for_each(normed_a, "tp").reshape(512, -1)

    normed_b = rms_rows(expert_input_rows, expert_norm_scale)
    route_weight = 2.5 * router_weights / jnp.sum(router_weights, axis=1, keepdims=True)
    token_count, top_count = routes.shape
    expert_count = lax.axis_size(EP) * lax.axis_size("tp")
    capacity = 2 * token_count * top_count // expert_count
    slots = expert_count * capacity
    chosen = routes.reshape(-1)
    onehot = (chosen[:, None] == jnp.arange(expert_count, dtype=jnp.int32)[None, :]).astype(BF)
    pairs = token_count * top_count
    lower = (jnp.arange(pairs)[:, None] > jnp.arange(pairs)[None, :]).astype(BF)
    counts = jnp.dot(lower, onehot, preferred_element_type=F32)
    rank = jnp.sum(counts * onehot, axis=1).astype(jnp.int32)
    slot_index = (chosen * capacity + rank).reshape(token_count, top_count)
    slot_ids = jnp.arange(slots, dtype=jnp.int32)[None, :]
    hit0 = slot_index[:, 0:1] == slot_ids
    hit1 = slot_index[:, 1:2] == slot_ids
    place = (hit0 | hit1).astype(BF)
    outgoing = lax.dot_general(place, normed_b, (((0,), (0,)), ((), ())), preferred_element_type=F32)
    outgoing = outgoing.astype(BF).reshape(expert_count, capacity, -1)
    arrived = lax.all_to_all(outgoing, EP_TP, split_axis=0, concat_axis=0, tiled=True)
    flat_rows = arrived.reshape(slots, -1)

    eb = jnp.repeat(erase_bias_table, 64).reshape(1, 256)
    out_l, rt, selft, tl = pl.pallas_call(
        mixer_kernel,
        out_shape=(
            jax.ShapeDtypeStruct((512, 256), F32),
            jax.ShapeDtypeStruct((512, 256), BF),
            jax.ShapeDtypeStruct((512, 256), F32),
            jax.ShapeDtypeStruct((128, 256), BF),
        ),
        in_specs=vspec(9),
        out_specs=tuple(vspec(4)),
        scratch_shapes=[
            VMEM((512, 1280), F32),
            VMEM((512, 256), BF),
            VMEM((1024, 256), BF),
            VMEM((1024, 256), F32),
            VMEM((64, 256), F32),
        ],
        cost_estimate=pl.CostEstimate(flops=6_000_000_000, bytes_accessed=10_000_000, transcendentals=0),
        name="mixer_local",
    )(row_piece, receive_weight, key_weight, value_weight, decay_weight, erase_weight,
      decay_bias_table, eb, self_token_scale.reshape(1, 256))

    enter = pl.pallas_call(
        state_kernel,
        out_shape=jax.ShapeDtypeStruct((64, 256), BF),
        in_specs=vspec(1),
        out_specs=vspec(1)[0],
        scratch_shapes=[
            VMEM((128, 256), BF),
            VMEM((128, 256), BF),
            VMEM((4, 128, 256), BF),
            VMEM((128, 256), BF),
            VMEM((4, 128, 256), BF),
            pltpu.SemaphoreType.DMA, pltpu.SemaphoreType.DMA,
            pltpu.SemaphoreType.DMA((4,)), pltpu.SemaphoreType.DMA((4,)),
            pltpu.SemaphoreType.DMA((4,)), pltpu.SemaphoreType.DMA((4,)),
        ],
        compiler_params=pltpu.CompilerParams(collective_id=0, has_side_effects=True),
        cost_estimate=pl.CostEstimate(flops=4_000_000_000, bytes_accessed=1_000_000, transcendentals=0),
        name="state_exchange",
    )(tl)

    partial = pl.pallas_call(
        finish_kernel,
        out_shape=jax.ShapeDtypeStruct((512, 2048), BF),
        in_specs=vspec(6),
        out_specs=vspec(1)[0],
        scratch_shapes=[VMEM((512, 256), BF)],
        cost_estimate=pl.CostEstimate(flops=2_000_000_000, bytes_accessed=4_000_000, transcendentals=0),
        name="mixer_finish",
    )(out_l, rt, selft, enter, head_norm_scale.reshape(1, 256), output_weight)
    pieces = lax.all_to_all(partial.reshape(4, 128, 2048), "tp", split_axis=0, concat_axis=0, tiled=True)
    mixer_output = pieces.astype(F32).sum(axis=0).astype(BF)

    gate_part, up_part, down_part = routed_gate_weight[0], routed_up_weight[0], routed_down_weight[0]
    expert_hidden = (
        jax.nn.silu(jnp.dot(flat_rows, gate_part, preferred_element_type=F32))
        * jnp.dot(flat_rows, up_part, preferred_element_type=F32)
    ).astype(BF)
    result = jnp.dot(expert_hidden, down_part, preferred_element_type=F32).astype(BF)
    returned = lax.all_to_all(
        result.reshape(expert_count, capacity, -1), EP_TP, split_axis=0, concat_axis=0, tiled=True
    )
    back_rows = returned.reshape(slots, -1)
    weights = jnp.where(hit0, route_weight[:, 0:1], 0.0) + jnp.where(hit1, route_weight[:, 1:2], 0.0)
    whi, wlo = split2(weights)
    routed = jnp.dot(whi, back_rows, preferred_element_type=F32) + jnp.dot(
        wlo, back_rows, preferred_element_type=F32
    )
    shared_hidden = (
        jax.nn.silu(jnp.dot(normed_b, common_gate_weight, preferred_element_type=F32))
        * jnp.dot(normed_b, common_up_weight, preferred_element_type=F32)
    ).astype(BF)
    shared_term = jnp.dot(shared_hidden, common_down_weight, preferred_element_type=F32)
    mixed_b = (routed + shared_term).astype(BF)
    return (mixer_output, mixed_b)


def solution(mesh):
    split = Mesh(mesh.devices.reshape(4, 4, 2, mesh.shape["tp"]), ("ep_0", "ep_1", "ep_2", "tp"))
    in_specs = (
        P(EP_TP, None), P(), P(EP, "tp"), P("tp"),
        P(None, "tp"), P(None, "tp"), P(None, "tp"), P(None, "tp"), P(None, "tp"),
        P("tp", None), P("tp"), P("tp", None),
        P(EP_TP, None), P(), P(EP_TP, None), P(EP_TP, None),
        P(EP_TP, None, None), P(EP_TP, None, None), P(EP_TP, None, None),
        P(), P(), P(),
    )
    out_specs = (P(EP_TP, None), P(EP_TP, None))
    return jax.shard_map(
        per_device, mesh=split, in_specs=in_specs, out_specs=out_specs, check_vma=False
    )
```

```python
import functools

import jax
import jax.numpy as jnp
from jax import lax
from jax.experimental import pallas as pl
from jax.experimental.pallas import tpu as pltpu
from jax.sharding import Mesh
from jax.sharding import PartitionSpec as P

EP = ("ep_0", "ep_1", "ep_2")
EP_TP = ("ep_0", "ep_1", "ep_2", "tp")
MESH = pl.DeviceIdType.MESH
BF = jnp.bfloat16
F32 = jnp.float32
VMEM = pltpu.VMEM
CHUNK = 64
PAIR = 128


def mm(a, b):
    return lax.dot_general(a, b, (((1,), (0,)), ((), ())), preferred_element_type=F32)


def mm_t(a, b):
    return lax.dot_general(a, b, (((1,), (1,)), ((), ())), preferred_element_type=F32)


def mm_tn(a, b):
    return lax.dot_general(a, b, (((0,), (0,)), ((), ())), preferred_element_type=F32)


def split2(x):
    hi = x.astype(BF)
    lo = (x - hi.astype(F32)).astype(BF)
    return hi, lo


def iota(shape, dim):
    return lax.broadcasted_iota(jnp.int32, shape, dim)


def pair_mask():
    return (iota((PAIR, PAIR), 0) // 64) == (iota((PAIR, PAIR), 1) // 64)


def block_diag(x, mask):
    return jnp.concatenate([x, x], axis=0) * mask


def head_sums(x, mask):
    hi, lo = split2(x)
    return mm(hi, mask) + mm(lo, mask)


def mixer_kernel(
    pr_ref, db_ref, eb_ref, st_ref, after_ref,
    out_ref, rt_ref, self_ref, tl_ref,
    r_s, e_s, l_s, d_s,
):
    n_rows = pr_ref.shape[0]
    n_chunks = n_rows // CHUNK
    group = 4
    mask_b = pair_mask()
    mask = mask_b.astype(F32).astype(BF)

    t_i = iota((CHUNK, PAIR), 0)
    s_i = iota((CHUNK, PAIR), 1) % 64
    strict = t_i > s_i
    causal = t_i >= s_i
    eye = (t_i == s_i).astype(F32)
    lane_lo = iota((CHUNK, PAIR), 1) < 64
    tril = (iota((CHUNK, CHUNK), 0) >= iota((CHUNK, CHUNK), 1)).astype(F32).astype(BF)

    def do_group(g, carry):
        units = []
        for cc in range(group):
            for p in range(2):
                r0 = pl.multiple_of((g * group + cc) * CHUNK, CHUNK)
                rows = pl.ds(r0, CHUNK)
                lanes = slice(p * PAIR, (p + 1) * PAIR)
                col = lambda j: pr_ref[rows, j * 256 + p * PAIR : j * 256 + (p + 1) * PAIR]
                r, k, v, dp, ep = (col(j) for j in range(5))
                db = db_ref[rows, :]
                db = jnp.where(lane_lo, db[:, 2 * p : 2 * p + 1], db[:, 2 * p + 1 : 2 * p + 2])
                ld = -0.6065306597126334 / (1.0 + jnp.exp(-(dp + db)))
                er = 1.0 / (1.0 + jnp.exp(-(ep + eb_ref[:, lanes])))
                u = k * lax.rsqrt(head_sums(k * k, mask) + 1e-06)
                self_ref[rows, lanes] = head_sums(r * k * st_ref[:, lanes], mask) * v
                hi, lo = split2(ld)
                cum = mm(tril, hi) + mm(tril, lo)
                end = cum[CHUNK - 1 : CHUNK, :]
                eci = jnp.exp(-cum)
                a = (-u * jnp.exp(cum - ld)).astype(BF)
                ri = r * jnp.exp(cum)
                ue = u * er
                b = (ue * eci).astype(BF)
                ko = (k * eci).astype(BF)
                tail = jnp.exp(end - cum)
                bt = (ue * tail).astype(BF)
                kt = (k * tail).astype(BF)
                ar = jnp.concatenate([a, ri.astype(BF)], axis=0)
                m13 = mm_t(ar, block_diag(b, mask))
                m24 = mm_t(ar, block_diag(ko, mask))
                m1 = jnp.where(strict, m13[:CHUNK], 0.0)
                m3 = jnp.where(causal, m13[CHUNK:], 0.0).astype(BF)
                m24 = jnp.concatenate(
                    [jnp.where(strict, m24[:CHUNK], 0.0), jnp.where(causal, m24[CHUNK:], 0.0)], axis=0
                ).astype(BF)
                vb = v.astype(BF)
                mv = mm(m24, block_diag(vb, mask))
                x = eye + jnp.where((t_i // 2) == (s_i // 2), m1, 0.0)
                units.append(
                    dict(rows=rows, lanes=lanes, p=p, r0=r0, a=a, ri=ri, m1=m1, m3=m3, mv=mv, x=x,
                         bt=bt, kt=kt, vb=vb, end=end)
                )
        size = 2
        while size < CHUNK:
            corner = ((t_i // (2 * size)) == (s_i // (2 * size))) & ((t_i // size) != (s_i // size))
            for n in units:
                xb = n["x"].astype(BF)
                n["xb"] = xb
                c = jnp.where(corner, n["m1"], 0.0).astype(BF)
                n["y"] = mm(xb, block_diag(c, mask)).astype(BF)
            for n in units:
                n["x"] = n["x"] + mm(n["y"], block_diag(n["xb"], mask))
            size *= 2
        for n in units:
            right = jnp.concatenate(
                [block_diag(n["a"], mask), block_diag(n["mv"][:CHUNK].astype(BF), mask)], axis=1
            )
            n["pq"] = mm(n["x"].astype(BF), right).astype(BF)
        for n in units:
            pb, qb = n["pq"][:, :PAIR], n["pq"][:, PAIR:]
            m3pq = mm(n["m3"], jnp.concatenate([block_diag(pb, mask), block_diag(qb, mask)], axis=1))
            r_s[n["rows"], n["lanes"]] = (n["ri"] + m3pq[:, :PAIR]).astype(BF)
            out_ref[n["rows"], n["lanes"]] = m3pq[:, PAIR:] + n["mv"][CHUNK:]
            big = pl.ds(pl.multiple_of(n["r0"] * 2, PAIR), PAIR)
            e_s[big, n["lanes"]] = (mm_tn(pb, n["bt"]) * mask).astype(BF)
            left = jnp.concatenate([qb, n["vb"]], axis=0)
            right = jnp.concatenate([n["bt"], n["kt"]], axis=0)
            l_s[big, n["lanes"]] = mm_tn(left, right) * mask
            small = pl.ds(pl.multiple_of(n["r0"] // 8, 8), 8)
            d_s[small, n["lanes"]] = jnp.broadcast_to(jnp.exp(n["end"]), (8, PAIR))
        return carry

    lax.fori_loop(0, n_chunks // group, do_group, 0)

    eye2 = (iota((PAIR, PAIR), 0) == iota((PAIR, PAIR), 1)).astype(F32)
    state = [jnp.concatenate([jnp.zeros((PAIR, PAIR), F32), eye2], axis=0) for _ in range(2)]
    for c in range(n_chunks):
        rows = slice(c * CHUNK, (c + 1) * CHUNK)
        big = slice(c * PAIR, (c + 1) * PAIR)
        for p in range(2):
            lanes = slice(p * PAIR, (p + 1) * PAIR)
            sb = state[p].astype(BF)
            o = mm_t(r_s[rows, lanes], sb)
            out_ref[rows, lanes] = out_ref[rows, lanes] + o[:, :PAIR]
            rt_ref[rows, lanes] = o[:, PAIR:].astype(BF)
            decayed = state[p] * d_s[c * 8 : c * 8 + 1, lanes]
            moved = mm(sb, e_s[big, lanes])
            state[p] = decayed + moved
            state[p] = jnp.concatenate([state[p][:PAIR] + l_s[big, lanes], state[p][PAIR:]], axis=0)
    for p in range(2):
        lanes = slice(p * PAIR, (p + 1) * PAIR)
        tl_ref[0:64, lanes] = (state[p][PAIR : PAIR + 64] + state[p][PAIR + 64 :]).astype(BF)
        tl_ref[64:128, lanes] = (state[p][0:64] + state[p][64:128]).astype(BF)


def state_kernel(tl_ref, enter_ref, cbuf, ysend, ybuf, zsend, zbuf, cs, cr, ys, yr, zs, zr):
    z, y, c = lax.axis_index("ep_0"), lax.axis_index("ep_1"), lax.axis_index("ep_2")
    barrier = pltpu.get_barrier_semaphore()
    pl.semaphore_signal(barrier, inc=1, device_id={"ep_2": 1 - c}, device_id_type=MESH)
    for d in range(1, 4):
        pl.semaphore_signal(barrier, inc=1, device_id={"ep_1": (y + d) % 4}, device_id_type=MESH)
        pl.semaphore_signal(barrier, inc=1, device_id={"ep_0": (z + d) % 4}, device_id_type=MESH)
    pl.semaphore_wait(barrier, 7)
    mask = pair_mask().astype(F32).astype(BF)

    def times(left, t):
        return jnp.concatenate(
            [mm(left[:, q * PAIR : (q + 1) * PAIR].astype(BF),
                block_diag(t[:, q * PAIR : (q + 1) * PAIR].astype(BF), mask)) for q in range(2)],
            axis=1,
        )

    def compose(early, late):
        joined = times(early, late[:64])
        return jnp.concatenate([joined[:64], joined[64:] + late[64:]], axis=0)

    cp = pltpu.make_async_remote_copy(
        src_ref=tl_ref, dst_ref=cbuf, send_sem=cs, recv_sem=cr,
        device_id={"ep_2": 1 - c}, device_id_type=MESH)
    cp.start()
    cp.wait()
    mine = tl_ref[...].astype(F32)
    other = cbuf[...].astype(F32)
    first = jnp.where(c == 0, mine, other)
    second = jnp.where(c == 0, other, mine)

    def exchange(value, send, buf, ss, rs, axis, me):
        send[...] = value.astype(BF)
        copies = []
        for d in range(1, 4):
            cp = pltpu.make_async_remote_copy(
                src_ref=send, dst_ref=buf.at[d], send_sem=ss.at[d], recv_sem=rs.at[d],
                device_id={axis: (me + d) % 4}, device_id_type=MESH)
            cp.start()
            copies.append(cp)
        buf[0] = value.astype(BF)
        for cp in copies:
            cp.wait()

    exchange(compose(first, second), ysend, ybuf, ys, yr, "ep_1", y)
    run = ybuf[y % 4].astype(F32)
    ident = (iota((64, 256), 0) == iota((64, 256), 1) % 64).astype(F32)
    before = jnp.concatenate([ident, jnp.zeros((64, 256), F32)], axis=0)
    for j in range(1, 4):
        before = jnp.where(y == j, run, before)
        run = compose(run, ybuf[(y - j + 4) % 4].astype(F32))
    exchange(run, zsend, zbuf, zs, zr, "ep_0", z)
    state = jnp.zeros((64, 256), F32)
    enter = state
    for j in range(0, 3):
        piece = zbuf[(z - j + 4) % 4].astype(F32)
        state = (times(state, piece[:64]) if j else 0.0) + piece[64:]
        enter = jnp.where(z == j + 1, state, enter)
    enter = times(enter, before[:64]) + before[64:]
    enter = jnp.where(c == 0, enter, times(enter, first[:64]) + first[64:])
    enter_ref[...] = enter.astype(BF)


def finish_kernel(
    out_ref, rt_ref, self_ref, enter_ref, gain_ref, w_hbm, res_ref,
    heads, landed, w_s, w_sem, ss, rs,
):
    t = lax.axis_index("tp")
    load = pltpu.make_async_copy(w_hbm, w_s, w_sem)
    load.start()
    barrier = pltpu.get_barrier_semaphore()
    for d in range(1, 4):
        pl.semaphore_signal(barrier, inc=1, device_id={"tp": (t + d) % 4}, device_id_type=MESH)
    mask = pair_mask().astype(F32).astype(BF)
    for p in range(2):
        lanes = slice(p * PAIR, (p + 1) * PAIR)
        ent = block_diag(enter_ref[:, lanes], mask)
        o = out_ref[:, lanes] + mm_t(rt_ref[:, lanes], ent)
        o = o - head_sums(o, mask) * (1.0 / 64)
        var = head_sums(o * o, mask) * (1.0 / 64)
        h = o * lax.rsqrt(var + 0.00064) * gain_ref[:, lanes] + self_ref[:, lanes]
        heads[:, lanes] = h.astype(BF)
    pl.semaphore_wait(barrier, 3)
    copies = []
    for d in (2, 1, 3):
        peer = (t + d) % 4
        cp = pltpu.make_async_remote_copy(
            src_ref=heads.at[pl.ds(pl.multiple_of(peer * 128, 128), 128)], dst_ref=landed.at[d],
            send_sem=ss.at[d], recv_sem=rs.at[d], device_id={"tp": peer}, device_id_type=MESH)
        cp.start()
        copies.append(cp)
    load.wait()
    own = heads[pl.ds(pl.multiple_of(t * 128, 128), 128), :]
    for cp in copies:
        cp.wait()
    for j in range(4):
        cols = slice(j * 512, (j + 1) * 512)
        total = mm(own, w_s[t, :, cols])
        for d in range(1, 4):
            total = total + mm(landed[d], w_s[(t + 4 - d) % 4, :, cols])
        res_ref[:, cols] = total.astype(BF)


def prep_kernel(a_ref, ga_ref, b_ref, gb_ref, routes_ref, rw_ref, na_ref, nb_ref, msg_ref, w_ref):
    for x_ref, g_ref, o_ref in ((a_ref, ga_ref, na_ref), (b_ref, gb_ref, nb_ref)):
        x = x_ref[...].astype(F32)
        inverse = lax.rsqrt(jnp.mean(x * x, axis=1, keepdims=True) + 1e-06)
        o_ref[...] = (x * inverse * g_ref[...]).astype(BF)
    n = 128
    c0 = routes_ref[:, 0:1].astype(F32)
    c1 = routes_ref[:, 1:2].astype(F32)
    lane = iota((n, n), 1)
    lane_f = lane.astype(F32)
    oh0 = (c0 == lane_f).astype(F32)
    oh1 = (c1 == lane_f).astype(F32)
    lower = (iota((n, n), 0) > lane).astype(F32).astype(BF)
    counts = mm(lower, (oh0 + oh1).astype(BF))
    s0 = c0 * 4.0 + jnp.sum(counts * oh0, axis=1, keepdims=True)
    s1 = c1 * 4.0 + jnp.sum(counts * oh1, axis=1, keepdims=True)
    rw = rw_ref[...]
    rw = 2.5 * rw / (rw[:, 0:1] + rw[:, 1:2])
    slot = iota((n, 512), 1).astype(F32)
    w = jnp.where(s0 == slot, rw[:, 0:1], 0.0) + jnp.where(s1 == slot, rw[:, 1:2], 0.0)
    hi, lo = split2(w)
    w_ref[0:n, :] = hi
    w_ref[n:, :] = lo
    turned = jnp.where(lane == 0, s0, jnp.where(lane == 1, s1, 0.0)).T
    r0, r1 = turned[0:1, :], turned[1:2, :]
    nb = nb_ref[...]
    pieces = jnp.concatenate([nb[:, q * 512 : (q + 1) * 512] for q in range(4)], axis=0)
    row = iota((256, n), 0)
    for i in range(8):
        ident = ((i * 16 + row // 16) * 4 + row % 4).astype(F32)
        hit = jnp.where((r0 == ident) | (r1 == ident), 1.0, 0.0)
        piece = (row // 4) % 4
        oh = jnp.concatenate([jnp.where(piece == q, hit, 0.0).astype(BF) for q in range(4)], axis=1)
        msg_ref[i * 16 : (i + 1) * 16] = mm(oh, pieces).astype(BF).reshape(16, 16, 512)


def order_mask(back):
    r, l = iota((256, 256), 0), iota((256, 256), 1)
    if back:
        r, l = l, r
    want = ((l // 4) % 4 == r // 64) & (l // 16 == (r % 64) // 4) & (l % 4 == r % 4)
    return want.astype(F32).astype(BF)


def unpack_rows(msg_ref, x_ref):
    order = order_mask(False)
    for i in range(8):
        rows = mm(order, msg_ref[i * 16 : (i + 1) * 16].reshape(256, 512)).astype(BF)
        for q in range(4):
            x_ref[i * 64 : (i + 1) * 64, q * 512 : (q + 1) * 512] = rows[q * 64 : (q + 1) * 64]


def ring_kernel(x_ref, wr_ref, wk_ref, wv_ref, wd_ref, we_ref, pr_ref, held, ss, rs, fs, fr):
    t = lax.axis_index("tp")
    right, left = (t + 1) % 4, (t + 3) % 4
    barrier = pltpu.get_barrier_semaphore()
    for q in (left, right):
        pl.semaphore_signal(barrier, inc=1, device_id={"tp": q}, device_id_type=MESH)
    pl.semaphore_wait(barrier, 2)
    n = 4
    step = 128 // n
    rows = lambda k: pl.ds(k * step, step)
    own = {}
    for i in range(n):
        for slot, k, peer in ((0, i, right), (1, (i + n // 2) % n, left)):
            cp = pltpu.make_async_remote_copy(
                src_ref=x_ref.at[rows(k)], dst_ref=held.at[slot, rows(k)],
                send_sem=ss.at[slot * n + k], recv_sem=rs.at[slot * n + k],
                device_id={"tp": peer}, device_id_type=MESH)
            cp.start()
            own[slot, k] = cp

    def project(block, who):
        at = pl.ds(pl.multiple_of(who * 128, 128), 128)
        for j, w in enumerate((wr_ref, wk_ref, wv_ref, wd_ref, we_ref)):
            pr_ref[at, j * 256 : (j + 1) * 256] = mm(block, w[...])

    project(x_ref[...], t)
    passed = []
    for i in range(n // 2):
        for slot, k, peer in ((0, i, right), (1, i + n // 2, left)):
            own[slot, k].wait_recv()
            cp = pltpu.make_async_remote_copy(
                src_ref=held.at[slot, rows(k)], dst_ref=held.at[2, rows(k)],
                send_sem=fs.at[k], recv_sem=fr.at[k],
                device_id={"tp": peer}, device_id_type=MESH)
            cp.start()
            passed.append(cp)
    for i in range(n // 2):
        own[0, i + n // 2].wait_recv()
        own[1, i].wait_recv()
    project(held[0], left)
    project(held[1], right)
    for cp in passed:
        cp.wait()
    project(held[2], (t + 2) % 4)
    for cp in own.values():
        cp.wait_send()


def expert_kernel(
    msg_ref, g_hbm, u_hbm, d_hbm, w_hbm, after_ref, res_ref, wall_hbm,
    x_s, g_s, u_s, d_s, h_s, w_s, g_sem, u_sem, d_sem, w_sem, ss, rs, fs, fr, cs, cr,
):
    t, c = lax.axis_index("tp"), lax.axis_index("ep_2")
    right, left = (t + 1) % 4, (t + 3) % 4
    barrier = pltpu.get_barrier_semaphore()
    for q in (left, right):
        pl.semaphore_signal(barrier, inc=1, device_id={"tp": q}, device_id_type=MESH)
    pl.semaphore_signal(barrier, inc=1, device_id={"ep_2": 1 - c}, device_id_type=MESH)
    loads = []
    for j in range(4):
        for src, dst, sem in ((g_hbm, g_s, g_sem), (u_hbm, u_s, u_sem)):
            cp = pltpu.make_async_copy(src.at[:, j * 256 : (j + 1) * 256], dst.at[j], sem.at[j])
            cp.start()
            loads.append(cp)
    own_w = pltpu.make_async_copy(w_hbm, w_s, w_sem.at[0])
    own_w.start()
    for j in range(4):
        pltpu.make_async_copy(d_hbm.at[:, j * 512 : (j + 1) * 512], d_s.at[j], d_sem.at[j]).start()
    pl.semaphore_wait(barrier, 3)
    own_w.wait()
    keep = pltpu.make_async_copy(w_s, wall_hbm.at[t], w_sem.at[1])
    keep.start()
    n = 2
    step = 64
    rows = lambda k: pl.ds(pl.multiple_of(c * 128 + k * step, step), step)
    own = {}
    for i in range(n):
        for slot, k, peer in ((0, i, right), (1, 1 - i, left)):
            cp = pltpu.make_async_remote_copy(
                src_ref=w_s.at[rows(k)], dst_ref=wall_hbm.at[t, rows(k)],
                send_sem=ss.at[slot * n + k], recv_sem=rs.at[slot * n + k],
                device_id={"tp": peer}, device_id_type=MESH)
            cp.start()
            own[slot, k] = cp
    unpack_rows(msg_ref, x_s)

    def hidden(j, carry):
        pltpu.make_async_copy(g_s.at[j], g_s.at[j], g_sem.at[j]).wait()
        pltpu.make_async_copy(u_s.at[j], u_s.at[j], u_sem.at[j]).wait()
        gate = mm(x_s[...], g_s[j])
        up = mm(x_s[...], u_s[j])
        h_s[j] = (gate / (1.0 + jnp.exp(-gate)) * up).astype(BF)
        return carry

    lax.fori_loop(0, 4, hidden, 0)
    passed = []
    for slot, k, peer, who in ((0, 0, right, left), (1, 1, left, right)):
        own[slot, k].wait_recv()
        cp = pltpu.make_async_remote_copy(
            src_ref=wall_hbm.at[who, rows(k)], dst_ref=wall_hbm.at[who, rows(k)],
            send_sem=fs.at[k], recv_sem=fr.at[k],
            device_id={"tp": peer}, device_id_type=MESH)
        cp.start()
        passed.append(cp)
    back = order_mask(True)
    for i in range(8):
        out = []
        for j in range(4):
            if i == 0:
                pltpu.make_async_copy(d_s.at[j], d_s.at[j], d_sem.at[j]).wait()
            acc = None
            for f in range(4):
                part = mm(h_s[f, i * 64 : (i + 1) * 64, :], d_s[j, f * 256 : (f + 1) * 256, :])
                acc = part if acc is None else acc + part
            out.append(acc.astype(BF))
        rows_out = jnp.concatenate(out, axis=0)
        res_ref[i * 16 : (i + 1) * 16] = mm(back, rows_out).astype(BF).reshape(16, 16, 512)
    own[0, 1].wait_recv()
    own[1, 0].wait_recv()
    shared = []
    half = pl.ds(pl.multiple_of(c * 128, 128), 128)

    def to_partner(i, who):
        cp = pltpu.make_async_remote_copy(
            src_ref=wall_hbm.at[who, half], dst_ref=wall_hbm.at[who, half],
            send_sem=cs.at[i], recv_sem=cr.at[i],
            device_id={"ep_2": 1 - c}, device_id_type=MESH)
        cp.start()
        shared.append(cp)

    to_partner(0, left)
    to_partner(1, right)
    for cp in passed:
        cp.wait()
    to_partner(2, (t + 2) % 4)
    for cp in own.values():
        cp.wait_send()
    keep.wait()
    for cp in shared:
        cp.wait()


def combine_kernel(msg_ref, w_ref, shared_ref, res_ref, x_s):
    unpack_rows(msg_ref, x_s)
    for j in range(4):
        cols = slice(j * 512, (j + 1) * 512)
        both = mm(w_ref[...], x_s[:, cols])
        res_ref[:, cols] = (both[:128] + both[128:] + shared_ref[:, cols]).astype(BF)


def vspec(n):
    return [pl.BlockSpec(memory_space=VMEM)] * n


def per_device(
    mixer_input_rows, mixer_norm_scale, decay_bias_table, erase_bias_table,
    receive_weight, key_weight, value_weight, decay_weight, erase_weight,
    self_token_scale, head_norm_scale, output_weight,
    expert_input_rows, expert_norm_scale, routes, router_weights,
    routed_gate_weight, routed_up_weight, routed_down_weight,
    common_gate_weight, common_up_weight, common_down_weight,
):
    any_spec = pl.BlockSpec(memory_space=pl.ANY)
    sds = jax.ShapeDtypeStruct
    dma = pltpu.SemaphoreType.DMA
    normed_a, normed_b, outgoing, weights = pl.pallas_call(
        prep_kernel,
        out_shape=(
            sds((128, 2048), BF), sds((128, 2048), BF), sds((128, 16, 512), BF), sds((256, 512), BF),
        ),
        in_specs=vspec(6),
        out_specs=tuple(vspec(4)),
        cost_estimate=pl.CostEstimate(flops=1_000_000_000, bytes_accessed=5_000_000, transcendentals=0),
        name="prep",
    )(mixer_input_rows, mixer_norm_scale.reshape(1, -1), expert_input_rows,
      expert_norm_scale.reshape(1, -1), routes, router_weights)
    arrived = lax.all_to_all(outgoing, EP_TP, split_axis=0, concat_axis=0, tiled=True)

    projected = pl.pallas_call(
        ring_kernel,
        out_shape=sds((512, 1280), F32),
        in_specs=vspec(6),
        out_specs=vspec(1)[0],
        scratch_shapes=[VMEM((3, 128, 2048), BF), dma((8,)), dma((8,)), dma((4,)), dma((4,))],
        compiler_params=pltpu.CompilerParams(collective_id=1, has_side_effects=True),
        cost_estimate=pl.CostEstimate(flops=12_000_000_000, bytes_accessed=8_000_000, transcendentals=0),
        name="ring_project",
    )(normed_a, receive_weight, key_weight, value_weight, decay_weight, erase_weight)

    result, w_all = pl.pallas_call(
        expert_kernel,
        out_shape=(sds((128, 16, 512), BF), sds((4, 256, 2048), BF)),
        in_specs=vspec(1) + [any_spec] * 5,
        out_specs=(vspec(1)[0], any_spec),
        scratch_shapes=[
            VMEM((512, 2048), BF),
            VMEM((4, 2048, 256), BF), VMEM((4, 2048, 256), BF), VMEM((4, 1024, 512), BF),
            VMEM((4, 512, 256), BF), VMEM((256, 2048), BF),
            dma((4,)), dma((4,)), dma((4,)), dma((2,)),
            dma((4,)), dma((4,)), dma((2,)), dma((2,)), dma((3,)), dma((3,)),
        ],
        compiler_params=pltpu.CompilerParams(collective_id=2, has_side_effects=True),
        cost_estimate=pl.CostEstimate(flops=8_000_000_000, bytes_accessed=16_000_000, transcendentals=0),
        name="experts",
    )(arrived, routed_gate_weight[0], routed_up_weight[0], routed_down_weight[0], output_weight, projected)
    returned = lax.all_to_all(result, EP_TP, split_axis=0, concat_axis=0, tiled=True)

    eb = jnp.repeat(erase_bias_table, 64).reshape(1, 256)
    out_l, rt, selft, tl = pl.pallas_call(
        mixer_kernel,
        out_shape=(sds((512, 256), F32), sds((512, 256), BF), sds((512, 256), F32), sds((128, 256), BF)),
        in_specs=vspec(4) + [any_spec],
        out_specs=tuple(vspec(4)),
        scratch_shapes=[VMEM((512, 256), BF), VMEM((1024, 256), BF), VMEM((1024, 256), F32), VMEM((64, 256), F32)],
        cost_estimate=pl.CostEstimate(flops=6_000_000_000, bytes_accessed=6_000_000, transcendentals=0),
        name="mixer_local",
    )(projected, decay_bias_table, eb, self_token_scale.reshape(1, 256), w_all)

    enter = pl.pallas_call(
        state_kernel,
        out_shape=sds((64, 256), BF),
        in_specs=vspec(1),
        out_specs=vspec(1)[0],
        scratch_shapes=[
            VMEM((128, 256), BF), VMEM((128, 256), BF), VMEM((4, 128, 256), BF),
            VMEM((128, 256), BF), VMEM((4, 128, 256), BF),
            dma, dma, dma((4,)), dma((4,)), dma((4,)), dma((4,)),
        ],
        compiler_params=pltpu.CompilerParams(collective_id=0, has_side_effects=True),
        cost_estimate=pl.CostEstimate(flops=6_000_000_000, bytes_accessed=1_000_000, transcendentals=0),
        name="state_exchange",
    )(tl)

    mixer_output = pl.pallas_call(
        finish_kernel,
        out_shape=sds((128, 2048), BF),
        in_specs=vspec(5) + [any_spec],
        out_specs=vspec(1)[0],
        scratch_shapes=[
            VMEM((512, 256), BF), VMEM((4, 128, 256), BF), VMEM((4, 256, 2048), BF),
            dma, dma((4,)), dma((4,)),
        ],
        compiler_params=pltpu.CompilerParams(collective_id=3, has_side_effects=True),
        cost_estimate=pl.CostEstimate(flops=5_000_000_000, bytes_accessed=6_000_000, transcendentals=0),
        name="mixer_finish",
    )(out_l, rt, selft, enter, head_norm_scale.reshape(1, 256), w_all)

    shared_hidden = (
        jax.nn.silu(jnp.dot(normed_b, common_gate_weight, preferred_element_type=F32))
        * jnp.dot(normed_b, common_up_weight, preferred_element_type=F32)
    ).astype(BF)
    shared_term = jnp.dot(shared_hidden, common_down_weight, preferred_element_type=F32)
    mixed_b = pl.pallas_call(
        combine_kernel,
        out_shape=sds((128, 2048), BF),
        in_specs=vspec(3),
        out_specs=vspec(1)[0],
        scratch_shapes=[VMEM((512, 2048), BF)],
        cost_estimate=pl.CostEstimate(flops=1_000_000_000, bytes_accessed=4_000_000, transcendentals=0),
        name="combine",
    )(returned, weights, shared_term)
    return (mixer_output, mixed_b)


def solution(mesh):
    split = Mesh(mesh.devices.reshape(4, 4, 2, mesh.shape["tp"]), ("ep_0", "ep_1", "ep_2", "tp"))
    in_specs = (
        P(EP_TP, None), P(), P(EP, "tp"), P("tp"),
        P(None, "tp"), P(None, "tp"), P(None, "tp"), P(None, "tp"), P(None, "tp"),
        P("tp", None), P("tp"), P("tp", None),
        P(EP_TP, None), P(), P(EP_TP, None), P(EP_TP, None),
        P(EP_TP, None, None), P(EP_TP, None, None), P(EP_TP, None, None),
        P(), P(), P(),
    )
    out_specs = (P(EP_TP, None), P(EP_TP, None))
    return jax.shard_map(
        per_device, mesh=split, in_specs=in_specs, out_specs=out_specs, check_vma=False
    )
```

```python
import functools

import jax
import jax.numpy as jnp
from jax import lax
from jax.experimental import pallas as pl
from jax.experimental.pallas import tpu as pltpu
from jax.sharding import Mesh
from jax.sharding import PartitionSpec as P

EP = ("ep_0", "ep_1", "ep_2")
EP_TP = ("ep_0", "ep_1", "ep_2", "tp")
MESH = pl.DeviceIdType.MESH
BF = jnp.bfloat16
F32 = jnp.float32
VMEM = pltpu.VMEM
CHUNK = 64
PAIR = 128


def mm(a, b):
    return lax.dot_general(a, b, (((1,), (0,)), ((), ())), preferred_element_type=F32)


def mm_t(a, b):
    return lax.dot_general(a, b, (((1,), (1,)), ((), ())), preferred_element_type=F32)


def mm_tn(a, b):
    return lax.dot_general(a, b, (((0,), (0,)), ((), ())), preferred_element_type=F32)


def split2(x):
    hi = x.astype(BF)
    lo = (x - hi.astype(F32)).astype(BF)
    return hi, lo


def iota(shape, dim):
    return lax.broadcasted_iota(jnp.int32, shape, dim)


def pair_mask():
    return (iota((PAIR, PAIR), 0) // 64) == (iota((PAIR, PAIR), 1) // 64)


def block_diag(x, mask):
    return jnp.concatenate([x, x], axis=0) * mask


def head_sums(x, mask):
    hi, lo = split2(x)
    return mm(hi, mask) + mm(lo, mask)


def split3(x):
    hi = x.astype(BF)
    rest = x - hi.astype(F32)
    mid = rest.astype(BF)
    return jnp.concatenate([hi, mid, (rest - mid.astype(F32)).astype(BF)], axis=0)


def mixer_body(pr_ref, db_ref, eb_ref, st_ref, out_ref, rt_ref, self_ref, tl_ref, r_s, e_s, l_s, d_s, db_s):
    n_rows = pr_ref.shape[1]
    n_chunks = n_rows // CHUNK
    group = 4
    mask_b = pair_mask()
    mask = mask_b.astype(F32).astype(BF)

    t_i = iota((CHUNK, PAIR), 0)
    s_i = iota((CHUNK, PAIR), 1) % 64
    strict = t_i > s_i
    causal = t_i >= s_i
    eye = (t_i == s_i).astype(F32)
    lane_lo = iota((CHUNK, PAIR), 1) < 64
    heads_of = (iota((12, 256), 0) % 4 == iota((12, 256), 1) // 64).astype(F32).astype(BF)
    db_s[...] = mm_tn(split3(db_ref[...]), heads_of)
    twice = jnp.concatenate([st_ref[...], st_ref[...]], axis=1)
    st = [jnp.where(lane_lo[0:1], twice[2 * p : 2 * p + 1], twice[2 * p + 1 : 2 * p + 2]) for p in range(2)]
    eb = [jnp.where(lane_lo[0:1], eb_ref[0:1, 2 * p : 2 * p + 1], eb_ref[0:1, 2 * p + 1 : 2 * p + 2]) for p in range(2)]
    tril = (iota((CHUNK, CHUNK), 0) >= iota((CHUNK, CHUNK), 1)).astype(F32).astype(BF)

    def do_group(g, carry):
        units = []
        for cc in range(group):
            for p in range(2):
                r0 = pl.multiple_of((g * group + cc) * CHUNK, CHUNK)
                rows = pl.ds(r0, CHUNK)
                lanes = slice(p * PAIR, (p + 1) * PAIR)
                col = lambda j: pr_ref[j, rows, lanes]
                r, k, v, dp, ep = (col(j) for j in range(5))
                ld = -0.6065306597126334 / (1.0 + jnp.exp(-(dp + db_s[rows, lanes])))
                er = 1.0 / (1.0 + jnp.exp(-(ep + eb[p])))
                u = k * lax.rsqrt(head_sums(k * k, mask) + 1e-06)
                self_ref[rows, lanes] = head_sums(r * k * st[p], mask) * v
                hi, lo = split2(ld)
                cum = mm(tril, hi) + mm(tril, lo)
                end = cum[CHUNK - 1 : CHUNK, :]
                eci = jnp.exp(-cum)
                a = (-u * jnp.exp(cum - ld)).astype(BF)
                ri = r * jnp.exp(cum)
                ue = u * er
                b = (ue * eci).astype(BF)
                ko = (k * eci).astype(BF)
                tail = jnp.exp(end - cum)
                bt = (ue * tail).astype(BF)
                kt = (k * tail).astype(BF)
                ar = jnp.concatenate([a, ri.astype(BF)], axis=0)
                m13 = mm_t(ar, block_diag(b, mask))
                m24 = mm_t(ar, block_diag(ko, mask))
                m1 = jnp.where(strict, m13[:CHUNK], 0.0)
                m3 = jnp.where(causal, m13[CHUNK:], 0.0).astype(BF)
                m24 = jnp.concatenate(
                    [jnp.where(strict, m24[:CHUNK], 0.0), jnp.where(causal, m24[CHUNK:], 0.0)], axis=0
                ).astype(BF)
                vb = v.astype(BF)
                mv = mm(m24, block_diag(vb, mask))
                x = eye + jnp.where((t_i // 2) == (s_i // 2), m1, 0.0)
                units.append(
                    dict(rows=rows, lanes=lanes, p=p, r0=r0, a=a, ri=ri, m1=m1, m3=m3, mv=mv, x=x,
                         bt=bt, kt=kt, vb=vb, end=end)
                )
        size = 2
        while size < CHUNK:
            corner = ((t_i // (2 * size)) == (s_i // (2 * size))) & ((t_i // size) != (s_i // size))
            for n in units:
                xb = n["x"].astype(BF)
                n["xb"] = xb
                c = jnp.where(corner, n["m1"], 0.0).astype(BF)
                n["y"] = mm(xb, block_diag(c, mask)).astype(BF)
            for n in units:
                n["x"] = n["x"] + mm(n["y"], block_diag(n["xb"], mask))
            size *= 2
        for n in units:
            right = jnp.concatenate(
                [block_diag(n["a"], mask), block_diag(n["mv"][:CHUNK].astype(BF), mask)], axis=1
            )
            n["pq"] = mm(n["x"].astype(BF), right).astype(BF)
        for n in units:
            pb, qb = n["pq"][:, :PAIR], n["pq"][:, PAIR:]
            m3pq = mm(n["m3"], jnp.concatenate([block_diag(pb, mask), block_diag(qb, mask)], axis=1))
            r_s[n["rows"], n["lanes"]] = (n["ri"] + m3pq[:, :PAIR]).astype(BF)
            out_ref[n["rows"], n["lanes"]] = m3pq[:, PAIR:] + n["mv"][CHUNK:]
            big = pl.ds(pl.multiple_of(n["r0"] * 2, PAIR), PAIR)
            e_s[big, n["lanes"]] = (mm_tn(pb, n["bt"]) * mask).astype(BF)
            left = jnp.concatenate([qb, n["vb"]], axis=0)
            right = jnp.concatenate([n["bt"], n["kt"]], axis=0)
            l_s[big, n["lanes"]] = mm_tn(left, right) * mask
            small = pl.ds(pl.multiple_of(n["r0"] // 8, 8), 8)
            d_s[small, n["lanes"]] = jnp.broadcast_to(jnp.exp(n["end"]), (8, PAIR))
        return carry

    lax.fori_loop(0, n_chunks // group, do_group, 0)

    eye2 = (iota((PAIR, PAIR), 0) == iota((PAIR, PAIR), 1)).astype(F32)
    state = [jnp.concatenate([jnp.zeros((PAIR, PAIR), F32), eye2], axis=0) for _ in range(2)]
    for c in range(n_chunks):
        rows = slice(c * CHUNK, (c + 1) * CHUNK)
        big = slice(c * PAIR, (c + 1) * PAIR)
        for p in range(2):
            lanes = slice(p * PAIR, (p + 1) * PAIR)
            sb = state[p].astype(BF)
            o = mm_t(r_s[rows, lanes], sb)
            out_ref[rows, lanes] = out_ref[rows, lanes] + o[:, :PAIR]
            rt_ref[rows, lanes] = o[:, PAIR:].astype(BF)
            decayed = state[p] * d_s[c * 8 : c * 8 + 1, lanes]
            moved = mm(sb, e_s[big, lanes])
            state[p] = decayed + moved
            state[p] = jnp.concatenate([state[p][:PAIR] + l_s[big, lanes], state[p][PAIR:]], axis=0)
    for p in range(2):
        lanes = slice(p * PAIR, (p + 1) * PAIR)
        tl_ref[0:64, lanes] = (state[p][PAIR : PAIR + 64] + state[p][PAIR + 64 :]).astype(BF)
        tl_ref[64:128, lanes] = (state[p][0:64] + state[p][64:128]).astype(BF)


def mixer_kernel(
    pr_ref, db_ref, eb_ref, st_ref, s0_hbm, s1_hbm,
    out_ref, rt_ref, self_ref, enter_ref, t0_hbm, t1_hbm,
    r_s, e_s, l_s, d_s, db_s, tl, hop, xs, xr, lsem, *state_scratch,
):
    z, y, c = lax.axis_index("ep_0"), lax.axis_index("ep_1"), lax.axis_index("ep_2")
    t = lax.axis_index("tp")
    takes = [pltpu.make_async_copy(s_hbm.at[:, :, c * 4 + t], hop.at[i], lsem.at[i])
             for i, s_hbm in enumerate((s0_hbm, s1_hbm))]
    for cp in takes:
        cp.start()
    signal_all(
        [{"ep_2": (c + dc) % 2, "tp": (t + dt) % 4} for dc in range(2) for dt in range(4) if dc or dt]
        + [{"ep_1": (y + d) % 4} for d in range(1, 4)]
        + [{"ep_0": (z + d) % 4} for d in range(1, 4)]
    )
    moves = []
    for dt in (1, 3, 2, 0):
        for dc in range(2):
            if not (dt or dc):
                continue
            pc, pt = (c + dc) % 2, (t + dt) % 4
            for i, (s_hbm, t_hbm) in enumerate(((s0_hbm, t0_hbm), (s1_hbm, t1_hbm))):
                at = i * 8 + dc * 4 + dt
                moves.append(
                    send(s_hbm.at[:, :, pc * 4 + pt], t_hbm.at[c * 4 + t], xs.at[at], xr.at[at],
                         {"ep_2": pc, "tp": pt}))
    for cp in takes:
        cp.wait()
    puts = [pltpu.make_async_copy(hop.at[i], t_hbm.at[c * 4 + t], lsem.at[i])
            for i, t_hbm in enumerate((t0_hbm, t1_hbm))]
    for cp in puts:
        cp.start()
    mixer_body(pr_ref, db_ref, eb_ref, st_ref, out_ref, rt_ref, self_ref, tl, r_s, e_s, l_s, d_s, db_s)
    state_body(tl, enter_ref, *state_scratch)
    for cp in puts + moves:
        cp.wait()


def state_body(tl_ref, enter_ref, cbuf, ysend, ybuf, zsend, zbuf, cs, cr, ys, yr, zs, zr):
    z, y, c = lax.axis_index("ep_0"), lax.axis_index("ep_1"), lax.axis_index("ep_2")
    mask = pair_mask().astype(F32).astype(BF)

    def times(left, t):
        return jnp.concatenate(
            [mm(left[:, q * PAIR : (q + 1) * PAIR].astype(BF),
                block_diag(t[:, q * PAIR : (q + 1) * PAIR].astype(BF), mask)) for q in range(2)],
            axis=1,
        )

    def compose(early, late):
        joined = times(early, late[:64])
        return jnp.concatenate([joined[:64], joined[64:] + late[64:]], axis=0)

    cp = pltpu.make_async_remote_copy(
        src_ref=tl_ref, dst_ref=cbuf, send_sem=cs, recv_sem=cr,
        device_id={"ep_2": 1 - c}, device_id_type=MESH)
    cp.start()
    cp.wait()
    mine = tl_ref[...].astype(F32)
    other = cbuf[...].astype(F32)
    first = jnp.where(c == 0, mine, other)
    second = jnp.where(c == 0, other, mine)

    def exchange(value, send, buf, ss, rs, axis, me):
        send[...] = value.astype(BF)
        copies = []
        for d in range(1, 4):
            cp = pltpu.make_async_remote_copy(
                src_ref=send, dst_ref=buf.at[d], send_sem=ss.at[d], recv_sem=rs.at[d],
                device_id={axis: (me + d) % 4}, device_id_type=MESH)
            cp.start()
            copies.append(cp)
        buf[0] = value.astype(BF)
        for cp in copies:
            cp.wait()

    exchange(compose(first, second), ysend, ybuf, ys, yr, "ep_1", y)
    run = ybuf[y % 4].astype(F32)
    ident = (iota((64, 256), 0) == iota((64, 256), 1) % 64).astype(F32)
    before = jnp.concatenate([ident, jnp.zeros((64, 256), F32)], axis=0)
    for j in range(1, 4):
        before = jnp.where(y == j, run, before)
        run = compose(run, ybuf[(y - j + 4) % 4].astype(F32))
    exchange(run, zsend, zbuf, zs, zr, "ep_0", z)
    state = jnp.zeros((64, 256), F32)
    enter = state
    for j in range(0, 3):
        piece = zbuf[(z - j + 4) % 4].astype(F32)
        state = (times(state, piece[:64]) if j else 0.0) + piece[64:]
        enter = jnp.where(z == j + 1, state, enter)
    enter = times(enter, before[:64]) + before[64:]
    enter = jnp.where(c == 0, enter, times(enter, first[:64]) + first[64:])
    enter_ref[...] = enter.astype(BF)


def finish_kernel(
    out_ref, rt_ref, self_ref, enter_ref, gain_ref, w_hbm, near_hbm, far_hbm, other_hbm, res_ref,
    heads, landed, w_s, w_sem, ss, rs,
):
    t, c = lax.axis_index("tp"), lax.axis_index("ep_2")
    mine = pl.ds(pl.multiple_of(c * 128, 128), 128)
    theirs = pl.ds(pl.multiple_of((1 - c) * 128, 128), 128)
    loads = [pltpu.make_async_copy(w_hbm, w_s.at[t], w_sem.at[0])]
    for i, src in enumerate((near_hbm.at[0], near_hbm.at[1], far_hbm)):
        who = (t + (3, 1, 2)[i]) % 4
        loads.append(pltpu.make_async_copy(src, w_s.at[who, mine], w_sem.at[1 + i]))
        loads.append(pltpu.make_async_copy(other_hbm.at[i], w_s.at[who, theirs], w_sem.at[4 + i]))
    for cp in loads:
        cp.start()
    barrier = pltpu.get_barrier_semaphore()
    for d in range(1, 4):
        pl.semaphore_signal(barrier, inc=1, device_id={"tp": (t + d) % 4}, device_id_type=MESH)
    mask = pair_mask().astype(F32).astype(BF)
    for p in range(2):
        lanes = slice(p * PAIR, (p + 1) * PAIR)
        ent = block_diag(enter_ref[:, lanes], mask)
        o = out_ref[:, lanes] + mm_t(rt_ref[:, lanes], ent)
        o = o - head_sums(o, mask) * (1.0 / 64)
        var = head_sums(o * o, mask) * (1.0 / 64)
        h = o * lax.rsqrt(var + 0.00064) * gain_ref[:, lanes] + self_ref[:, lanes]
        heads[:, lanes] = h.astype(BF)
    pl.semaphore_wait(barrier, 3)
    copies = []
    for d in (2, 1, 3):
        peer = (t + d) % 4
        copies.append(
            send(heads.at[pl.ds(pl.multiple_of(peer * 128, 128), 128)], landed.at[d], ss.at[d], rs.at[d],
                 {"tp": peer}))
    for cp in loads:
        cp.wait()
    own = heads[pl.ds(pl.multiple_of(t * 128, 128), 128), :]
    for cp in copies:
        cp.wait()
    for j in range(4):
        cols = slice(j * 512, (j + 1) * 512)
        total = mm(own, w_s[t, :, cols])
        for d in range(1, 4):
            total = total + mm(landed[d], w_s[(t + 4 - d) % 4, :, cols])
        res_ref[:, cols] = total.astype(BF)


def prep_kernel(a_ref, ga_ref, b_ref, gb_ref, routes_ref, rw_ref, na_ref, nb_ref, m0_ref, m1_ref, w_ref):
    for x_ref, g_ref, o_ref in ((a_ref, ga_ref, na_ref), (b_ref, gb_ref, nb_ref)):
        x = x_ref[...].astype(F32)
        inverse = lax.rsqrt(jnp.mean(x * x, axis=1, keepdims=True) + 1e-06)
        o_ref[...] = (x * inverse * g_ref[...]).astype(BF)
    n = 128
    chosen = routes_ref[...].astype(F32)
    c0, c1 = chosen[0:1, :], chosen[1:2, :]
    sub = iota((n, n), 0)
    sub_f = sub.astype(F32)
    oh0 = jnp.where(c0 == sub_f, 1.0, 0.0)
    oh1 = jnp.where(c1 == sub_f, 1.0, 0.0)
    before = (sub < iota((n, n), 1)).astype(F32).astype(BF)
    counts = mm((oh0 + oh1).astype(BF), before)
    s0 = c0 * 4.0 + jnp.sum(counts * oh0, axis=0, keepdims=True)
    s1 = c1 * 4.0 + jnp.sum(counts * oh1, axis=0, keepdims=True)
    rw = rw_ref[...]
    rw = 2.5 * rw / (rw[0:1, :] + rw[1:2, :])
    slot = iota((512, n), 0).astype(F32)
    w = jnp.where(s0 == slot, rw[0:1, :], 0.0) + jnp.where(s1 == slot, rw[1:2, :], 0.0)
    hi, lo = split2(w)
    w_ref[:, 0:n] = hi
    w_ref[:, n:] = lo
    nb = nb_ref[...]
    pieces = jnp.concatenate([nb[:, q * 512 : (q + 1) * 512] for q in range(4)], axis=0)
    row = iota((256, n), 0)
    for i in range(8):
        ident = ((i * 16 + row // 16) * 4 + row % 4).astype(F32)
        hit = jnp.where((s0 == ident) | (s1 == ident), 1.0, 0.0)
        piece = (row // 4) % 4
        oh = jnp.concatenate([jnp.where(piece == q, hit, 0.0).astype(BF) for q in range(4)], axis=1)
        res = mm(oh, pieces).astype(BF)
        for h in range(2):
            z, y = i // 2, (i % 2) * 2 + h
            half = res[h * 128 : (h + 1) * 128]
            m0_ref[y, z] = half[:, :256].reshape(8, 16, 256)
            m1_ref[z, y] = half[:, 256:].reshape(8, 16, 256)


def order_mask(back):
    r, l = iota((256, 256), 0), iota((256, 256), 1)
    if back:
        r, l = l, r
    want = ((l // 4) % 4 == r // 64) & (l // 16 == (r % 64) // 4) & (l % 4 == r % 4)
    return want.astype(F32).astype(BF)


def unpack_block(order, block, x_ref, i):
    rows = mm(order, block).astype(BF)
    for q in range(4):
        x_ref[i * 64 : (i + 1) * 64, q * 512 : (q + 1) * 512] = rows[q * 64 : (q + 1) * 64]


def signal_all(peers):
    barrier = pltpu.get_barrier_semaphore()
    for peer in peers:
        pl.semaphore_signal(barrier, inc=1, device_id=peer, device_id_type=MESH)
    pl.semaphore_wait(barrier, len(peers))


def send(src, dst, ss, rs, peer):
    cp = pltpu.make_async_remote_copy(
        src_ref=src, dst_ref=dst, send_sem=ss, recv_sem=rs, device_id=peer, device_id_type=MESH)
    cp.start()
    return cp


def ring_kernel(
    x_ref, m0_ref, m1_ref, wr, wk, wv, wd, we, wo,
    pr_ref, s0_ref, s1_ref, near_ref,
    held, r0, r1, w_s, wsem, ss, rs, fs, fr, as_, ar, bs, br, os_, or_, lsem,
):
    z, y, t = lax.axis_index("ep_0"), lax.axis_index("ep_1"), lax.axis_index("tp")
    c = lax.axis_index("ep_2")
    right, left = (t + 1) % 4, (t + 3) % 4
    loads = []
    for j, w in enumerate((wr, wk, wv, wd, we)):
        cp = pltpu.make_async_copy(w, w_s.at[j], wsem.at[j])
        cp.start()
        loads.append(cp)
    signal_all(
        [{"tp": right}, {"tp": left}]
        + [{"ep_1": (y + d) % 4} for d in range(1, 4)]
        + [{"ep_0": (z + d) % 4} for d in range(1, 4)]
    )
    n = 4
    step = 128 // n
    rows = lambda k: pl.ds(k * step, step)
    own = {}
    first = []
    for i in range(n):
        for slot, k, peer in ((0, i, right), (1, (i + n // 2) % n, left)):
            own[slot, k] = send(
                x_ref.at[rows(k)], held.at[slot, rows(k)], ss.at[slot * n + k], rs.at[slot * n + k], {"tp": peer})
        if i == 0:
            for d in (1, 3, 2):
                first.append(send(m0_ref.at[(y + d) % 4], r0.at[y], as_.at[d], ar.at[d], {"ep_1": (y + d) % 4}))
                first.append(
                    send(m1_ref.at[(z + d) % 4], r1.at[z], as_.at[4 + d], ar.at[4 + d], {"ep_0": (z + d) % 4}))
    kept = [
        pltpu.make_async_copy(m0_ref.at[y], r0.at[y], lsem.at[0]),
        pltpu.make_async_copy(m1_ref.at[z], r1.at[z], lsem.at[1]),
    ]
    for cp in kept:
        cp.start()
    for cp in loads:
        cp.wait()

    def project(block, who):
        at = pl.ds(pl.multiple_of(who * 128, 128), 128)

        def one(j, carry):
            pr_ref[j, at, :] = mm(block, w_s[j])
            return carry

        lax.fori_loop(0, 5, one, 0)

    project(x_ref[...], t)
    passed = []
    for i in range(n // 2):
        for slot, k, peer in ((0, i, right), (1, i + n // 2, left)):
            own[slot, k].wait_recv()
            passed.append(
                send(held.at[slot, rows(k)], held.at[2, rows(k)], fs.at[k], fr.at[k], {"tp": peer}))
    half = pl.ds(pl.multiple_of(c * 128, 128), 128)
    outs = [
        send(wo.at[half], near_ref.at[0], os_.at[0], or_.at[0], {"tp": right}),
        send(wo.at[half], near_ref.at[1], os_.at[1], or_.at[1], {"tp": left}),
    ]
    for cp in kept:
        cp.wait()
    for cp in first:
        cp.wait()
    second = []
    for d in (1, 3, 2):
        second.append(
            send(r0.at[:, (z + d) % 4], s0_ref.at[z], bs.at[d], br.at[d], {"ep_0": (z + d) % 4}))
        second.append(
            send(r1.at[:, (y + d) % 4], s1_ref.at[y], bs.at[4 + d], br.at[4 + d], {"ep_1": (y + d) % 4}))
    kept = [
        pltpu.make_async_copy(r0.at[:, z], s0_ref.at[z], lsem.at[0]),
        pltpu.make_async_copy(r1.at[:, y], s1_ref.at[y], lsem.at[1]),
    ]
    for cp in kept:
        cp.start()
    for i in range(n // 2):
        own[0, i + n // 2].wait_recv()
        own[1, i].wait_recv()
    project(held[0], left)
    project(held[1], right)
    for cp in passed:
        cp.wait()
    project(held[2], (t + 2) % 4)
    for cp in own.values():
        cp.wait_send()
    for cp in kept + second + outs:
        cp.wait()


def expert_kernel(
    t0_ref, t1_ref, g_hbm, u_hbm, d_hbm, near_hbm, res_ref, far_hbm, other_hbm,
    x_s, g_s, u_s, d_s, h_s, g_sem, u_sem, d_sem, fs, fr, cs, cr,
):
    t, c = lax.axis_index("tp"), lax.axis_index("ep_2")
    right, left = (t + 1) % 4, (t + 3) % 4
    loads = []
    for j in range(4):
        for src, dst, sem in ((g_hbm, g_s, g_sem), (u_hbm, u_s, u_sem)):
            pltpu.make_async_copy(src.at[:, j * 256 : (j + 1) * 256], dst.at[j], sem.at[j]).start()
    for j in range(4):
        pltpu.make_async_copy(d_hbm.at[:, j * 512 : (j + 1) * 512], d_s.at[j], d_sem.at[j]).start()
    signal_all([{"tp": right}, {"tp": left}, {"ep_2": 1 - c}])
    passed = [
        send(near_hbm.at[0, 0:64], far_hbm.at[0:64], fs.at[0], fr.at[0], {"tp": right}),
        send(near_hbm.at[1, 64:128], far_hbm.at[64:128], fs.at[1], fr.at[1], {"tp": left}),
    ]
    shared = [send(near_hbm.at[i], other_hbm.at[i], cs.at[i], cr.at[i], {"ep_2": 1 - c}) for i in range(2)]
    order = order_mask(False)
    for i in range(8):
        one = t0_ref[i].reshape(256, 256)
        two = jnp.concatenate([t1_ref[i, y, z] for z in range(4) for y in range(4)], axis=0)
        unpack_block(order, jnp.concatenate([one, two], axis=1), x_s, i)

    def hidden(j, carry):
        pltpu.make_async_copy(g_s.at[j], g_s.at[j], g_sem.at[j]).wait()
        pltpu.make_async_copy(u_s.at[j], u_s.at[j], u_sem.at[j]).wait()
        gate = mm(x_s[...], g_s[j])
        up = mm(x_s[...], u_s[j])
        h_s[j] = (gate / (1.0 + jnp.exp(-gate)) * up).astype(BF)
        return carry

    lax.fori_loop(0, 4, hidden, 0)
    for j in range(4):
        pltpu.make_async_copy(d_s.at[j], d_s.at[j], d_sem.at[j]).wait()
    for j in range(4):
        acc = None
        for f in range(4):
            part = mm(h_s[f], d_s[j, f * 256 : (f + 1) * 256, :])
            acc = part if acc is None else acc + part
        x_s[:, j * 512 : (j + 1) * 512] = acc.astype(BF)
    back = order_mask(True)
    for i in range(8):
        rows_out = jnp.concatenate(
            [x_s[i * 64 : (i + 1) * 64, q * 512 : (q + 1) * 512] for q in range(4)], axis=0)
        units = mm(back, rows_out).astype(BF).reshape(16, 16, 512)
        for k in range(16):
            res_ref[k * 8 + i] = units[k]
    for cp in passed:
        cp.wait()
    shared.append(send(far_hbm, other_hbm.at[2], cs.at[2], cr.at[2], {"ep_2": 1 - c}))
    for cp in shared:
        cp.wait()


def combine_kernel(msg_ref, w_ref, shared_ref, res_ref, x_s):
    order = order_mask(False)
    for i in range(8):
        unpack_block(order, msg_ref[i * 16 : (i + 1) * 16].reshape(256, 512), x_s, i)
    for j in range(4):
        cols = slice(j * 512, (j + 1) * 512)
        both = mm_tn(w_ref[...], x_s[:, cols])
        res_ref[:, cols] = (both[:128] + both[128:] + shared_ref[:, cols]).astype(BF)


def vspec(n):
    return [pl.BlockSpec(memory_space=VMEM)] * n


def per_device(
    mixer_input_rows, mixer_norm_scale, decay_bias_table, erase_bias_table,
    receive_weight, key_weight, value_weight, decay_weight, erase_weight,
    self_token_scale, head_norm_scale, output_weight,
    expert_input_rows, expert_norm_scale, routes, router_weights,
    routed_gate_weight, routed_up_weight, routed_down_weight,
    common_gate_weight, common_up_weight, common_down_weight,
):
    any_spec = pl.BlockSpec(memory_space=pl.ANY)
    sds = jax.ShapeDtypeStruct
    dma = pltpu.SemaphoreType.DMA
    m_shape = sds((4, 4, 8, 16, 256), BF)
    normed_a, normed_b, m0, m1, weights = pl.pallas_call(
        prep_kernel,
        out_shape=(sds((128, 2048), BF), sds((128, 2048), BF), m_shape, m_shape, sds((512, 256), BF)),
        in_specs=vspec(6),
        out_specs=tuple(vspec(5)),
        cost_estimate=pl.CostEstimate(flops=1_000_000_000, bytes_accessed=5_000_000, transcendentals=0),
        name="prep",
    )(mixer_input_rows, mixer_norm_scale.reshape(1, -1), expert_input_rows,
      expert_norm_scale.reshape(1, -1), routes.T, router_weights.T)

    projected, s0, s1, near = pl.pallas_call(
        ring_kernel,
        out_shape=(sds((5, 512, 256), F32), m_shape, m_shape, sds((2, 128, 2048), BF)),
        in_specs=vspec(3) + [any_spec] * 6,
        out_specs=(vspec(1)[0], any_spec, any_spec, any_spec),
        scratch_shapes=[
            VMEM((3, 128, 2048), BF), VMEM((4, 4, 8, 16, 256), BF), VMEM((4, 4, 8, 16, 256), BF),
            VMEM((5, 2048, 256), BF), dma((5,)),
            dma((8,)), dma((8,)), dma((4,)), dma((4,)), dma((8,)), dma((8,)), dma((8,)), dma((8,)),
            dma((2,)), dma((2,)), dma((2,)),
        ],
        compiler_params=pltpu.CompilerParams(collective_id=1, has_side_effects=True),
        cost_estimate=pl.CostEstimate(flops=12_000_000_000, bytes_accessed=8_000_000, transcendentals=0),
        name="ring_project",
    )(normed_a, m0, m1, receive_weight, key_weight, value_weight, decay_weight, erase_weight, output_weight)

    t_shape = sds((8, 4, 4, 16, 256), BF)
    out_l, rt, selft, enter, t0, t1 = pl.pallas_call(
        mixer_kernel,
        out_shape=(sds((512, 256), F32), sds((512, 256), BF), sds((512, 256), F32), sds((64, 256), BF),
                   t_shape, t_shape),
        in_specs=vspec(4) + [any_spec] * 2,
        out_specs=tuple(vspec(4)) + (any_spec, any_spec),
        scratch_shapes=[
            VMEM((512, 256), BF), VMEM((1024, 256), BF), VMEM((1024, 256), F32), VMEM((64, 256), F32),
            VMEM((512, 256), F32), VMEM((128, 256), BF), VMEM((2, 4, 4, 16, 256), BF),
            dma((16,)), dma((16,)), dma((2,)),
            VMEM((128, 256), BF), VMEM((128, 256), BF), VMEM((4, 128, 256), BF),
            VMEM((128, 256), BF), VMEM((4, 128, 256), BF),
            dma, dma, dma((4,)), dma((4,)), dma((4,)), dma((4,)),
        ],
        compiler_params=pltpu.CompilerParams(collective_id=0, has_side_effects=True),
        cost_estimate=pl.CostEstimate(flops=6_000_000_000, bytes_accessed=6_000_000, transcendentals=0),
        name="mixer_state",
    )(projected, decay_bias_table.T, erase_bias_table.reshape(1, 4), self_token_scale, s0, s1)

    result, far, other = pl.pallas_call(
        expert_kernel,
        out_shape=(sds((128, 16, 512), BF), sds((128, 2048), BF), sds((3, 128, 2048), BF)),
        in_specs=vspec(2) + [any_spec] * 4,
        out_specs=(vspec(1)[0], any_spec, any_spec),
        scratch_shapes=[
            VMEM((512, 2048), BF),
            VMEM((4, 2048, 256), BF), VMEM((4, 2048, 256), BF), VMEM((4, 1024, 512), BF),
            VMEM((4, 512, 256), BF),
            dma((4,)), dma((4,)), dma((4,)), dma((2,)), dma((2,)), dma((3,)), dma((3,)),
        ],
        compiler_params=pltpu.CompilerParams(collective_id=2, has_side_effects=True),
        cost_estimate=pl.CostEstimate(flops=8_000_000_000, bytes_accessed=16_000_000, transcendentals=0),
        name="experts",
    )(t0, t1, routed_gate_weight[0], routed_up_weight[0], routed_down_weight[0], near)
    returned = lax.all_to_all(result, EP_TP, split_axis=0, concat_axis=0, tiled=True)

    mixer_output = pl.pallas_call(
        finish_kernel,
        out_shape=sds((128, 2048), BF),
        in_specs=vspec(5) + [any_spec] * 4,
        out_specs=vspec(1)[0],
        scratch_shapes=[
            VMEM((512, 256), BF), VMEM((4, 128, 256), BF), VMEM((4, 256, 2048), BF),
            dma((7,)), dma((4,)), dma((4,)),
        ],
        compiler_params=pltpu.CompilerParams(collective_id=3, has_side_effects=True),
        cost_estimate=pl.CostEstimate(flops=5_000_000_000, bytes_accessed=6_000_000, transcendentals=0),
        name="mixer_finish",
    )(out_l, rt, selft, enter, head_norm_scale.reshape(1, 256), output_weight, near, far, other)

    shared_hidden = (
        jax.nn.silu(jnp.dot(normed_b, common_gate_weight, preferred_element_type=F32))
        * jnp.dot(normed_b, common_up_weight, preferred_element_type=F32)
    ).astype(BF)
    shared_term = jnp.dot(shared_hidden, common_down_weight, preferred_element_type=F32)
    mixed_b = pl.pallas_call(
        combine_kernel,
        out_shape=sds((128, 2048), BF),
        in_specs=vspec(3),
        out_specs=vspec(1)[0],
        scratch_shapes=[VMEM((512, 2048), BF)],
        cost_estimate=pl.CostEstimate(flops=1_000_000_000, bytes_accessed=4_000_000, transcendentals=0),
        name="combine",
    )(returned, weights, shared_term)
    return (mixer_output, mixed_b)


def solution(mesh):
    split = Mesh(mesh.devices.reshape(4, 4, 2, mesh.shape["tp"]), ("ep_0", "ep_1", "ep_2", "tp"))
    in_specs = (
        P(EP_TP, None), P(), P(EP, "tp"), P("tp"),
        P(None, "tp"), P(None, "tp"), P(None, "tp"), P(None, "tp"), P(None, "tp"),
        P("tp", None), P("tp"), P("tp", None),
        P(EP_TP, None), P(), P(EP_TP, None), P(EP_TP, None),
        P(EP_TP, None, None), P(EP_TP, None, None), P(EP_TP, None, None),
        P(), P(), P(),
    )
    out_specs = (P(EP_TP, None), P(EP_TP, None))
    return jax.shard_map(
        per_device, mesh=split, in_specs=in_specs, out_specs=out_specs, check_vma=False
    )
```

```python
import functools

import jax
import jax.numpy as jnp
from jax import lax
from jax.experimental import pallas as pl
from jax.experimental.pallas import tpu as pltpu
from jax.sharding import Mesh
from jax.sharding import PartitionSpec as P

EP = ("ep_0", "ep_1", "ep_2")
EP_TP = ("ep_0", "ep_1", "ep_2", "tp")
MESH = pl.DeviceIdType.MESH
BF = jnp.bfloat16
F32 = jnp.float32
VMEM = pltpu.VMEM
CHUNK = 64
PAIR = 128


def mm(a, b):
    return lax.dot_general(a, b, (((1,), (0,)), ((), ())), preferred_element_type=F32)


def mm_t(a, b):
    return lax.dot_general(a, b, (((1,), (1,)), ((), ())), preferred_element_type=F32)


def mm_tn(a, b):
    return lax.dot_general(a, b, (((0,), (0,)), ((), ())), preferred_element_type=F32)


def split2(x):
    hi = x.astype(BF)
    lo = (x - hi.astype(F32)).astype(BF)
    return hi, lo


def iota(shape, dim):
    return lax.broadcasted_iota(jnp.int32, shape, dim)


def pair_mask():
    return (iota((PAIR, PAIR), 0) // 64) == (iota((PAIR, PAIR), 1) // 64)


def block_diag(x, mask):
    return jnp.concatenate([x, x], axis=0) * mask


def head_sums(x, mask):
    hi, lo = split2(x)
    return mm(hi, mask) + mm(lo, mask)


def split3(x):
    hi = x.astype(BF)
    rest = x - hi.astype(F32)
    mid = rest.astype(BF)
    return jnp.concatenate([hi, mid, (rest - mid.astype(F32)).astype(BF)], axis=0)


def mixer_body(pr_ref, db_ref, eb_ref, st_ref, out_ref, rt_ref, self_ref, tl_ref, r_s, e_s, l_s, d_s, db_s):
    n_rows = pr_ref.shape[1]
    n_chunks = n_rows // CHUNK
    group = 4
    mask_b = pair_mask()
    mask = mask_b.astype(F32).astype(BF)

    t_i = iota((CHUNK, PAIR), 0)
    s_i = iota((CHUNK, PAIR), 1) % 64
    strict = t_i > s_i
    causal = t_i >= s_i
    eye = (t_i == s_i).astype(F32)
    lane_lo = iota((CHUNK, PAIR), 1) < 64
    heads_of = (iota((12, 256), 0) % 4 == iota((12, 256), 1) // 64).astype(F32).astype(BF)
    db_s[...] = mm_tn(split3(db_ref[...]), heads_of)
    twice = jnp.concatenate([st_ref[...], st_ref[...]], axis=1)
    st = [jnp.where(lane_lo[0:1], twice[2 * p : 2 * p + 1], twice[2 * p + 1 : 2 * p + 2]) for p in range(2)]
    eb = [jnp.where(lane_lo[0:1], eb_ref[0:1, 2 * p : 2 * p + 1], eb_ref[0:1, 2 * p + 1 : 2 * p + 2]) for p in range(2)]
    tril = (iota((CHUNK, CHUNK), 0) >= iota((CHUNK, CHUNK), 1)).astype(F32).astype(BF)

    def do_group(g, carry):
        units = []
        for cc in range(group):
            for p in range(2):
                r0 = pl.multiple_of((g * group + cc) * CHUNK, CHUNK)
                rows = pl.ds(r0, CHUNK)
                lanes = slice(p * PAIR, (p + 1) * PAIR)
                col = lambda j: pr_ref[j, rows, lanes]
                r, k, v, dp, ep = (col(j) for j in range(5))
                ld = -0.6065306597126334 / (1.0 + jnp.exp(-(dp + db_s[rows, lanes])))
                er = 1.0 / (1.0 + jnp.exp(-(ep + eb[p])))
                u = k * lax.rsqrt(head_sums(k * k, mask) + 1e-06)
                self_ref[rows, lanes] = head_sums(r * k * st[p], mask) * v
                hi, lo = split2(ld)
                cum = mm(tril, hi) + mm(tril, lo)
                end = cum[CHUNK - 1 : CHUNK, :]
                eci = jnp.exp(-cum)
                a = (-u * jnp.exp(cum - ld)).astype(BF)
                ri = r * jnp.exp(cum)
                ue = u * er
                b = (ue * eci).astype(BF)
                ko = (k * eci).astype(BF)
                tail = jnp.exp(end - cum)
                bt = (ue * tail).astype(BF)
                kt = (k * tail).astype(BF)
                ar = jnp.concatenate([a, ri.astype(BF)], axis=0)
                m13 = mm_t(ar, block_diag(b, mask))
                m24 = mm_t(ar, block_diag(ko, mask))
                m1 = jnp.where(strict, m13[:CHUNK], 0.0)
                m3 = jnp.where(causal, m13[CHUNK:], 0.0).astype(BF)
                m24 = jnp.concatenate(
                    [jnp.where(strict, m24[:CHUNK], 0.0), jnp.where(causal, m24[CHUNK:], 0.0)], axis=0
                ).astype(BF)
                vb = v.astype(BF)
                mv = mm(m24, block_diag(vb, mask))
                x = eye + jnp.where((t_i // 2) == (s_i // 2), m1, 0.0)
                units.append(
                    dict(rows=rows, lanes=lanes, p=p, r0=r0, a=a, ri=ri, m1=m1, m3=m3, mv=mv, x=x,
                         bt=bt, kt=kt, vb=vb, end=end)
                )
        size = 2
        while size < CHUNK:
            corner = ((t_i // (2 * size)) == (s_i // (2 * size))) & ((t_i // size) != (s_i // size))
            for n in units:
                xb = n["x"].astype(BF)
                n["xb"] = xb
                c = jnp.where(corner, n["m1"], 0.0).astype(BF)
                n["y"] = mm(xb, block_diag(c, mask)).astype(BF)
            for n in units:
                n["x"] = n["x"] + mm(n["y"], block_diag(n["xb"], mask))
            size *= 2
        for n in units:
            right = jnp.concatenate(
                [block_diag(n["a"], mask), block_diag(n["mv"][:CHUNK].astype(BF), mask)], axis=1
            )
            n["pq"] = mm(n["x"].astype(BF), right).astype(BF)
        for n in units:
            pb, qb = n["pq"][:, :PAIR], n["pq"][:, PAIR:]
            m3pq = mm(n["m3"], jnp.concatenate([block_diag(pb, mask), block_diag(qb, mask)], axis=1))
            r_s[n["rows"], n["lanes"]] = (n["ri"] + m3pq[:, :PAIR]).astype(BF)
            out_ref[n["rows"], n["lanes"]] = m3pq[:, PAIR:] + n["mv"][CHUNK:]
            big = pl.ds(pl.multiple_of(n["r0"] * 2, PAIR), PAIR)
            e_s[big, n["lanes"]] = (mm_tn(pb, n["bt"]) * mask).astype(BF)
            left = jnp.concatenate([qb, n["vb"]], axis=0)
            right = jnp.concatenate([n["bt"], n["kt"]], axis=0)
            l_s[big, n["lanes"]] = mm_tn(left, right) * mask
            small = pl.ds(pl.multiple_of(n["r0"] // 8, 8), 8)
            d_s[small, n["lanes"]] = jnp.broadcast_to(jnp.exp(n["end"]), (8, PAIR))
        return carry

    lax.fori_loop(0, n_chunks // group, do_group, 0)

    eye2 = (iota((PAIR, PAIR), 0) == iota((PAIR, PAIR), 1)).astype(F32)
    state = [jnp.concatenate([jnp.zeros((PAIR, PAIR), F32), eye2], axis=0) for _ in range(2)]
    for c in range(n_chunks):
        rows = slice(c * CHUNK, (c + 1) * CHUNK)
        big = slice(c * PAIR, (c + 1) * PAIR)
        for p in range(2):
            lanes = slice(p * PAIR, (p + 1) * PAIR)
            sb = state[p].astype(BF)
            o = mm_t(r_s[rows, lanes], sb)
            out_ref[rows, lanes] = out_ref[rows, lanes] + o[:, :PAIR]
            rt_ref[rows, lanes] = o[:, PAIR:].astype(BF)
            decayed = state[p] * d_s[c * 8 : c * 8 + 1, lanes]
            moved = mm(sb, e_s[big, lanes])
            state[p] = decayed + moved
            state[p] = jnp.concatenate([state[p][:PAIR] + l_s[big, lanes], state[p][PAIR:]], axis=0)
    for p in range(2):
        lanes = slice(p * PAIR, (p + 1) * PAIR)
        tl_ref[0:64, lanes] = (state[p][PAIR : PAIR + 64] + state[p][PAIR + 64 :]).astype(BF)
        tl_ref[64:128, lanes] = (state[p][0:64] + state[p][64:128]).astype(BF)


def mixer_kernel(
    pr_ref, db_ref, eb_ref, st_ref, s0_hbm, s1_hbm,
    out_ref, rt_ref, self_ref, enter_ref, t0_hbm, t1_hbm,
    r_s, e_s, l_s, d_s, db_s, tl, hop, xs, xr, lsem, *state_scratch,
):
    z, y, c = lax.axis_index("ep_0"), lax.axis_index("ep_1"), lax.axis_index("ep_2")
    t = lax.axis_index("tp")
    takes = [pltpu.make_async_copy(s_hbm.at[:, :, c * 4 + t], hop.at[i], lsem.at[i])
             for i, s_hbm in enumerate((s0_hbm, s1_hbm))]
    for cp in takes:
        cp.start()
    signal_all(
        [{"ep_2": (c + dc) % 2, "tp": (t + dt) % 4} for dc in range(2) for dt in range(4) if dc or dt]
        + [{"ep_1": (y + d) % 4} for d in range(1, 4)]
        + [{"ep_0": (z + d) % 4} for d in range(1, 4)]
    )
    moves = []
    for dt in (1, 3, 2, 0):
        for dc in range(2):
            if not (dt or dc):
                continue
            pc, pt = (c + dc) % 2, (t + dt) % 4
            for i, (s_hbm, t_hbm) in enumerate(((s0_hbm, t0_hbm), (s1_hbm, t1_hbm))):
                at = i * 8 + dc * 4 + dt
                moves.append(
                    send(s_hbm.at[:, :, pc * 4 + pt], t_hbm.at[c * 4 + t], xs.at[at], xr.at[at],
                         {"ep_2": pc, "tp": pt}))
    for cp in takes:
        cp.wait()
    puts = [pltpu.make_async_copy(hop.at[i], t_hbm.at[c * 4 + t], lsem.at[i])
            for i, t_hbm in enumerate((t0_hbm, t1_hbm))]
    for cp in puts:
        cp.start()
    mixer_body(pr_ref, db_ref, eb_ref, st_ref, out_ref, rt_ref, self_ref, tl, r_s, e_s, l_s, d_s, db_s)
    state_body(tl, enter_ref, *state_scratch)
    for cp in puts + moves:
        cp.wait()


def state_body(tl_ref, enter_ref, cbuf, ysend, ybuf, zsend, zbuf, cs, cr, ys, yr, zs, zr):
    z, y, c = lax.axis_index("ep_0"), lax.axis_index("ep_1"), lax.axis_index("ep_2")
    mask = pair_mask().astype(F32).astype(BF)

    def times(left, t):
        return jnp.concatenate(
            [mm(left[:, q * PAIR : (q + 1) * PAIR].astype(BF),
                block_diag(t[:, q * PAIR : (q + 1) * PAIR].astype(BF), mask)) for q in range(2)],
            axis=1,
        )

    def compose(early, late):
        joined = times(early, late[:64])
        return jnp.concatenate([joined[:64], joined[64:] + late[64:]], axis=0)

    cp = pltpu.make_async_remote_copy(
        src_ref=tl_ref, dst_ref=cbuf, send_sem=cs, recv_sem=cr,
        device_id={"ep_2": 1 - c}, device_id_type=MESH)
    cp.start()
    cp.wait()
    mine = tl_ref[...].astype(F32)
    other = cbuf[...].astype(F32)
    first = jnp.where(c == 0, mine, other)
    second = jnp.where(c == 0, other, mine)

    def exchange(value, send, buf, ss, rs, axis, me):
        send[...] = value.astype(BF)
        copies = []
        for d in range(1, 4):
            cp = pltpu.make_async_remote_copy(
                src_ref=send, dst_ref=buf.at[d], send_sem=ss.at[d], recv_sem=rs.at[d],
                device_id={axis: (me + d) % 4}, device_id_type=MESH)
            cp.start()
            copies.append(cp)
        buf[0] = value.astype(BF)
        for cp in copies:
            cp.wait()

    exchange(compose(first, second), ysend, ybuf, ys, yr, "ep_1", y)
    run = ybuf[y % 4].astype(F32)
    ident = (iota((64, 256), 0) == iota((64, 256), 1) % 64).astype(F32)
    before = jnp.concatenate([ident, jnp.zeros((64, 256), F32)], axis=0)
    for j in range(1, 4):
        before = jnp.where(y == j, run, before)
        run = compose(run, ybuf[(y - j + 4) % 4].astype(F32))
    exchange(run, zsend, zbuf, zs, zr, "ep_0", z)
    state = jnp.zeros((64, 256), F32)
    enter = state
    for j in range(0, 3):
        piece = zbuf[(z - j + 4) % 4].astype(F32)
        state = (times(state, piece[:64]) if j else 0.0) + piece[64:]
        enter = jnp.where(z == j + 1, state, enter)
    enter = times(enter, before[:64]) + before[64:]
    enter = jnp.where(c == 0, enter, times(enter, first[:64]) + first[64:])
    enter_ref[...] = enter.astype(BF)


PARTS = ("xyz", "yzx", "zxy", "xyz")
SIZES = {"x": 8, "y": 4, "z": 4}


def part_shape(part, stage):
    names = part[:stage][::-1] + part[stage:]
    return tuple(SIZES[a] for a in names) + (16, 128)


def finish_kernel(
    out_ref, rt_ref, self_ref, enter_ref, gain_ref, nb_ref,
    p0, p1, p2, p3, w_hbm, near_hbm, far_hbm, other_hbm, cg_hbm, cu_hbm, cd_hbm,
    res_ref, shared_ref, q0, q1, q2, q3,
    heads, landed, w_s, cg, cu, cd, *rest,
):
    mids, (w_sem, c_sem, hs, hr, ss, rs, ls) = rest[:8], rest[8:]
    z, y, c = lax.axis_index("ep_0"), lax.axis_index("ep_1"), lax.axis_index("ep_2")
    t = lax.axis_index("tp")
    signal_all(
        [{"ep_2": (c + dc) % 2, "tp": (t + dt) % 4} for dc in range(2) for dt in range(4) if dc or dt]
        + [{"ep_1": (y + d) % 4} for d in range(1, 4)]
        + [{"ep_0": (z + d) % 4} for d in range(1, 4)]
    )
    refs = [
        (p0, mids[0], mids[1], q0), (p1, mids[2], mids[3], q1),
        (p2, mids[4], mids[5], q2), (p3, mids[6], mids[7], q3),
    ]

    def go(part, stage):
        src, dst = refs[part][stage], refs[part][stage + 1]
        axis = PARTS[part][stage]
        cut = lambda who: src.at[(slice(None),) * stage + (who,)]
        out = []
        if axis == "x":
            me = c * 4 + t
            for dt, dc in ((1, 0), (3, 1), (1, 1), (3, 0), (2, 0), (2, 1), (0, 1)):
                pc, pt = (c + dc) % 2, (t + dt) % 4
                at = dc * 4 + dt
                out.append(send(cut(pc * 4 + pt), dst.at[me], ss.at[part, stage, at], rs.at[part, stage, at],
                                {"ep_2": pc, "tp": pt}))
        else:
            name, me = ("ep_1", y) if axis == "y" else ("ep_0", z)
            for d in (1, 3, 2):
                peer = (me + d) % 4
                out.append(send(cut(peer), dst.at[me], ss.at[part, stage, d], rs.at[part, stage, d], {name: peer}))
        own = pltpu.make_async_copy(cut(me), dst.at[me], ls.at[part, stage])
        own.start()
        return out + [own]

    def finish(copies):
        for cp in copies:
            cp.wait()

    a0, b0, c0, d0 = go(0, 0), go(1, 0), go(2, 0), go(3, 0)
    shared_w = [pltpu.make_async_copy(src, dst, c_sem.at[i])
                for i, (src, dst) in enumerate(((cg_hbm, cg), (cu_hbm, cu), (cd_hbm, cd)))]
    mine = pl.ds(pl.multiple_of(c * 128, 128), 128)
    theirs = pl.ds(pl.multiple_of((1 - c) * 128, 128), 128)
    loads = [pltpu.make_async_copy(w_hbm, w_s.at[t], w_sem.at[0])]
    for i, src in enumerate((near_hbm.at[0], near_hbm.at[1], far_hbm)):
        who = (t + (3, 1, 2)[i]) % 4
        loads.append(pltpu.make_async_copy(src, w_s.at[who, mine], w_sem.at[1 + i]))
        loads.append(pltpu.make_async_copy(other_hbm.at[i], w_s.at[who, theirs], w_sem.at[4 + i]))
    for cp in shared_w + loads:
        cp.start()
    mask = pair_mask().astype(F32).astype(BF)
    for p in range(2):
        lanes = slice(p * PAIR, (p + 1) * PAIR)
        ent = block_diag(enter_ref[:, lanes], mask)
        o = out_ref[:, lanes] + mm_t(rt_ref[:, lanes], ent)
        o = o - head_sums(o, mask) * (1.0 / 64)
        var = head_sums(o * o, mask) * (1.0 / 64)
        h = o * lax.rsqrt(var + 0.00064) * gain_ref[:, lanes] + self_ref[:, lanes]
        heads[:, lanes] = h.astype(BF)
    copies = []
    for d in (2, 1, 3):
        peer = (t + d) % 4
        copies.append(
            send(heads.at[pl.ds(pl.multiple_of(peer * 128, 128), 128)], landed.at[d], hs.at[d], hr.at[d],
                 {"tp": peer}))
    finish(b0)
    b1 = go(1, 1)
    finish(c0)
    c1 = go(2, 1)
    finish(a0)
    a1 = go(0, 1)
    finish(shared_w)
    gate = mm(nb_ref[...], cg[...])
    hid = (gate / (1.0 + jnp.exp(-gate)) * mm(nb_ref[...], cu[...])).astype(BF)
    for j in range(4):
        cols = slice(j * 512, (j + 1) * 512)
        shared_ref[:, cols] = mm(hid, cd[:, cols])
    finish(d0)
    d1 = go(3, 1)
    finish(b1)
    b2 = go(1, 2)
    finish(a1)
    a2 = go(0, 2)
    finish(c1)
    c2 = go(2, 2)
    finish(d1)
    d2 = go(3, 2)
    finish(loads)
    own = heads[pl.ds(pl.multiple_of(t * 128, 128), 128), :]
    finish(copies)
    for j in range(4):
        cols = slice(j * 512, (j + 1) * 512)
        total = mm(own, w_s[t, :, cols])
        for d in range(1, 4):
            total = total + mm(landed[d], w_s[(t + 4 - d) % 4, :, cols])
        res_ref[:, cols] = total.astype(BF)
    for copies in (a2, b2, c2, d2):
        finish(copies)


def prep_kernel(a_ref, ga_ref, b_ref, gb_ref, routes_ref, rw_ref, na_ref, nb_ref, m0_ref, m1_ref, w_ref):
    for x_ref, g_ref, o_ref in ((a_ref, ga_ref, na_ref), (b_ref, gb_ref, nb_ref)):
        x = x_ref[...].astype(F32)
        inverse = lax.rsqrt(jnp.mean(x * x, axis=1, keepdims=True) + 1e-06)
        o_ref[...] = (x * inverse * g_ref[...]).astype(BF)
    n = 128
    chosen = routes_ref[...].astype(F32)
    c0, c1 = chosen[0:1, :], chosen[1:2, :]
    sub = iota((n, n), 0)
    sub_f = sub.astype(F32)
    oh0 = jnp.where(c0 == sub_f, 1.0, 0.0)
    oh1 = jnp.where(c1 == sub_f, 1.0, 0.0)
    before = (sub < iota((n, n), 1)).astype(F32).astype(BF)
    counts = mm((oh0 + oh1).astype(BF), before)
    s0 = c0 * 4.0 + jnp.sum(counts * oh0, axis=0, keepdims=True)
    s1 = c1 * 4.0 + jnp.sum(counts * oh1, axis=0, keepdims=True)
    rw = rw_ref[...]
    rw = 2.5 * rw / (rw[0:1, :] + rw[1:2, :])
    slot = iota((512, n), 0).astype(F32)
    w = jnp.where(s0 == slot, rw[0:1, :], 0.0) + jnp.where(s1 == slot, rw[1:2, :], 0.0)
    hi, lo = split2(w)
    w_ref[:, 0:n] = hi
    w_ref[:, n:] = lo
    nb = nb_ref[...]
    pieces = jnp.concatenate([nb[:, q * 512 : (q + 1) * 512] for q in range(4)], axis=0)
    row = iota((256, n), 0)
    for i in range(8):
        ident = ((i * 16 + row // 16) * 4 + row % 4).astype(F32)
        hit = jnp.where((s0 == ident) | (s1 == ident), 1.0, 0.0)
        piece = (row // 4) % 4
        oh = jnp.concatenate([jnp.where(piece == q, hit, 0.0).astype(BF) for q in range(4)], axis=1)
        res = mm(oh, pieces).astype(BF)
        for h in range(2):
            z, y = i // 2, (i % 2) * 2 + h
            half = res[h * 128 : (h + 1) * 128]
            m0_ref[y, z] = half[:, :256].reshape(8, 16, 256)
            m1_ref[z, y] = half[:, 256:].reshape(8, 16, 256)


def order_mask(back):
    r, l = iota((256, 256), 0), iota((256, 256), 1)
    if back:
        r, l = l, r
    want = ((l // 4) % 4 == r // 64) & (l // 16 == (r % 64) // 4) & (l % 4 == r % 4)
    return want.astype(F32).astype(BF)


def unpack_block(order, block, x_ref, i):
    rows = mm(order, block).astype(BF)
    for q in range(4):
        x_ref[i * 64 : (i + 1) * 64, q * 512 : (q + 1) * 512] = rows[q * 64 : (q + 1) * 64]


def signal_all(peers):
    barrier = pltpu.get_barrier_semaphore()
    for peer in peers:
        pl.semaphore_signal(barrier, inc=1, device_id=peer, device_id_type=MESH)
    pl.semaphore_wait(barrier, len(peers))


def send(src, dst, ss, rs, peer):
    cp = pltpu.make_async_remote_copy(
        src_ref=src, dst_ref=dst, send_sem=ss, recv_sem=rs, device_id=peer, device_id_type=MESH)
    cp.start()
    return cp


def ring_kernel(
    x_ref, m0_ref, m1_ref, wr, wk, wv, wd, we, wo,
    pr_ref, s0_ref, s1_ref, near_ref,
    held, r0, r1, w_s, wsem, ss, rs, fs, fr, as_, ar, bs, br, os_, or_, lsem,
):
    z, y, t = lax.axis_index("ep_0"), lax.axis_index("ep_1"), lax.axis_index("tp")
    c = lax.axis_index("ep_2")
    right, left = (t + 1) % 4, (t + 3) % 4
    loads = []
    for j, w in enumerate((wr, wk, wv, wd, we)):
        cp = pltpu.make_async_copy(w, w_s.at[j], wsem.at[j])
        cp.start()
        loads.append(cp)
    signal_all(
        [{"tp": right}, {"tp": left}]
        + [{"ep_1": (y + d) % 4} for d in range(1, 4)]
        + [{"ep_0": (z + d) % 4} for d in range(1, 4)]
    )
    n = 4
    step = 128 // n
    rows = lambda k: pl.ds(k * step, step)
    own = {}
    first = []
    for i in range(n):
        for slot, k, peer in ((0, i, right), (1, (i + n // 2) % n, left)):
            own[slot, k] = send(
                x_ref.at[rows(k)], held.at[slot, rows(k)], ss.at[slot * n + k], rs.at[slot * n + k], {"tp": peer})
        if i == 0:
            for d in (1, 3, 2):
                first.append(send(m0_ref.at[(y + d) % 4], r0.at[y], as_.at[d], ar.at[d], {"ep_1": (y + d) % 4}))
                first.append(
                    send(m1_ref.at[(z + d) % 4], r1.at[z], as_.at[4 + d], ar.at[4 + d], {"ep_0": (z + d) % 4}))
    kept = [
        pltpu.make_async_copy(m0_ref.at[y], r0.at[y], lsem.at[0]),
        pltpu.make_async_copy(m1_ref.at[z], r1.at[z], lsem.at[1]),
    ]
    for cp in kept:
        cp.start()
    for cp in loads:
        cp.wait()

    def project(block, who):
        at = pl.ds(pl.multiple_of(who * 128, 128), 128)

        def one(j, carry):
            pr_ref[j, at, :] = mm(block, w_s[j])
            return carry

        lax.fori_loop(0, 5, one, 0)

    project(x_ref[...], t)
    passed = []
    for i in range(n // 2):
        for slot, k, peer in ((0, i, right), (1, i + n // 2, left)):
            own[slot, k].wait_recv()
            passed.append(
                send(held.at[slot, rows(k)], held.at[2, rows(k)], fs.at[k], fr.at[k], {"tp": peer}))
    half = pl.ds(pl.multiple_of(c * 128, 128), 128)
    outs = [
        send(wo.at[half], near_ref.at[0], os_.at[0], or_.at[0], {"tp": right}),
        send(wo.at[half], near_ref.at[1], os_.at[1], or_.at[1], {"tp": left}),
    ]
    for cp in kept:
        cp.wait()
    for cp in first:
        cp.wait()
    second = []
    for d in (1, 3, 2):
        second.append(
            send(r0.at[:, (z + d) % 4], s0_ref.at[z], bs.at[d], br.at[d], {"ep_0": (z + d) % 4}))
        second.append(
            send(r1.at[:, (y + d) % 4], s1_ref.at[y], bs.at[4 + d], br.at[4 + d], {"ep_1": (y + d) % 4}))
    kept = [
        pltpu.make_async_copy(r0.at[:, z], s0_ref.at[z], lsem.at[0]),
        pltpu.make_async_copy(r1.at[:, y], s1_ref.at[y], lsem.at[1]),
    ]
    for cp in kept:
        cp.start()
    for i in range(n // 2):
        own[0, i + n // 2].wait_recv()
        own[1, i].wait_recv()
    project(held[0], left)
    project(held[1], right)
    for cp in passed:
        cp.wait()
    project(held[2], (t + 2) % 4)
    for cp in own.values():
        cp.wait_send()
    for cp in kept + second + outs:
        cp.wait()


def expert_kernel(
    t0_ref, t1_ref, g_hbm, u_hbm, d_hbm, near_hbm, p0_ref, p1_ref, p2_ref, p3_ref, far_hbm, other_hbm,
    x_s, g_s, u_s, d_s, h_s, g_sem, u_sem, d_sem, fs, fr, cs, cr,
):
    t, c = lax.axis_index("tp"), lax.axis_index("ep_2")
    right, left = (t + 1) % 4, (t + 3) % 4
    loads = []
    for j in range(4):
        for src, dst, sem in ((g_hbm, g_s, g_sem), (u_hbm, u_s, u_sem)):
            pltpu.make_async_copy(src.at[:, j * 256 : (j + 1) * 256], dst.at[j], sem.at[j]).start()
    for j in range(4):
        pltpu.make_async_copy(d_hbm.at[:, j * 512 : (j + 1) * 512], d_s.at[j], d_sem.at[j]).start()
    signal_all([{"tp": right}, {"tp": left}, {"ep_2": 1 - c}])
    passed = [
        send(near_hbm.at[0, 0:64], far_hbm.at[0:64], fs.at[0], fr.at[0], {"tp": right}),
        send(near_hbm.at[1, 64:128], far_hbm.at[64:128], fs.at[1], fr.at[1], {"tp": left}),
    ]
    shared = [send(near_hbm.at[i], other_hbm.at[i], cs.at[i], cr.at[i], {"ep_2": 1 - c}) for i in range(2)]
    order = order_mask(False)
    for i in range(8):
        one = t0_ref[i].reshape(256, 256)
        two = jnp.concatenate([t1_ref[i, y, z] for z in range(4) for y in range(4)], axis=0)
        unpack_block(order, jnp.concatenate([one, two], axis=1), x_s, i)

    def hidden(j, carry):
        pltpu.make_async_copy(g_s.at[j], g_s.at[j], g_sem.at[j]).wait()
        pltpu.make_async_copy(u_s.at[j], u_s.at[j], u_sem.at[j]).wait()
        gate = mm(x_s[...], g_s[j])
        up = mm(x_s[...], u_s[j])
        h_s[j] = (gate / (1.0 + jnp.exp(-gate)) * up).astype(BF)
        return carry

    lax.fori_loop(0, 4, hidden, 0)
    for j in range(4):
        pltpu.make_async_copy(d_s.at[j], d_s.at[j], d_sem.at[j]).wait()
    for j in range(4):
        acc = None
        for f in range(4):
            part = mm(h_s[f], d_s[j, f * 256 : (f + 1) * 256, :])
            acc = part if acc is None else acc + part
        x_s[:, j * 512 : (j + 1) * 512] = acc.astype(BF)
    back = order_mask(True)
    for i in range(8):
        rows_out = jnp.concatenate(
            [x_s[i * 64 : (i + 1) * 64, q * 512 : (q + 1) * 512] for q in range(4)], axis=0)
        units = mm(back, rows_out).astype(BF).reshape(16, 16, 512)
        for k in range(16):
            z, y = k // 4, k % 4
            p0_ref[i, y, z] = units[k, :, 0:128]
            p1_ref[y, z, i] = units[k, :, 128:256]
            p2_ref[z, i, y] = units[k, :, 256:384]
            p3_ref[i, y, z] = units[k, :, 384:512]
    for cp in passed:
        cp.wait()
    shared.append(send(far_hbm, other_hbm.at[2], cs.at[2], cr.at[2], {"ep_2": 1 - c}))
    for cp in shared:
        cp.wait()


def combine_kernel(q0, q1, q2, q3, w_ref, shared_ref, mixer_ref, pass_ref, res_ref, x_s):
    pass_ref[...] = mixer_ref[...]
    order = order_mask(False)
    for i in range(8):
        z, ys = i // 2, (2 * (i % 2), 2 * (i % 2) + 1)
        cols = [q0[z, ys[0] : ys[0] + 2].reshape(256, 128)]
        cols.append(jnp.concatenate([q1[x, z, y] for y in ys for x in range(8)], axis=0))
        cols.append(jnp.concatenate([q2[y, x, z] for y in ys for x in range(8)], axis=0))
        cols.append(q3[z, ys[0] : ys[0] + 2].reshape(256, 128))
        unpack_block(order, jnp.concatenate(cols, axis=1), x_s, i)
    for j in range(4):
        cols = slice(j * 512, (j + 1) * 512)
        both = mm_tn(w_ref[...], x_s[:, cols])
        res_ref[:, cols] = (both[:128] + both[128:] + shared_ref[:, cols]).astype(BF)


def vspec(n):
    return [pl.BlockSpec(memory_space=VMEM)] * n


def per_device(
    mixer_input_rows, mixer_norm_scale, decay_bias_table, erase_bias_table,
    receive_weight, key_weight, value_weight, decay_weight, erase_weight,
    self_token_scale, head_norm_scale, output_weight,
    expert_input_rows, expert_norm_scale, routes, router_weights,
    routed_gate_weight, routed_up_weight, routed_down_weight,
    common_gate_weight, common_up_weight, common_down_weight,
):
    any_spec = pl.BlockSpec(memory_space=pl.ANY)
    sds = jax.ShapeDtypeStruct
    dma = pltpu.SemaphoreType.DMA
    m_shape = sds((4, 4, 8, 16, 256), BF)
    normed_a, normed_b, m0, m1, weights = pl.pallas_call(
        prep_kernel,
        out_shape=(sds((128, 2048), BF), sds((128, 2048), BF), m_shape, m_shape, sds((512, 256), BF)),
        in_specs=vspec(6),
        out_specs=tuple(vspec(5)),
        cost_estimate=pl.CostEstimate(flops=1_000_000_000, bytes_accessed=5_000_000, transcendentals=0),
        name="prep",
    )(mixer_input_rows, mixer_norm_scale.reshape(1, -1), expert_input_rows,
      expert_norm_scale.reshape(1, -1), routes.T, router_weights.T)

    projected, s0, s1, near = pl.pallas_call(
        ring_kernel,
        out_shape=(sds((5, 512, 256), F32), m_shape, m_shape, sds((2, 128, 2048), BF)),
        in_specs=vspec(3) + [any_spec] * 6,
        out_specs=(vspec(1)[0], any_spec, any_spec, any_spec),
        scratch_shapes=[
            VMEM((3, 128, 2048), BF), VMEM((4, 4, 8, 16, 256), BF), VMEM((4, 4, 8, 16, 256), BF),
            VMEM((5, 2048, 256), BF), dma((5,)),
            dma((8,)), dma((8,)), dma((4,)), dma((4,)), dma((8,)), dma((8,)), dma((8,)), dma((8,)),
            dma((2,)), dma((2,)), dma((2,)),
        ],
        compiler_params=pltpu.CompilerParams(collective_id=1, has_side_effects=True),
        cost_estimate=pl.CostEstimate(flops=12_000_000_000, bytes_accessed=8_000_000, transcendentals=0),
        name="ring_project",
    )(normed_a, m0, m1, receive_weight, key_weight, value_weight, decay_weight, erase_weight, output_weight)

    t_shape = sds((8, 4, 4, 16, 256), BF)
    out_l, rt, selft, enter, t0, t1 = pl.pallas_call(
        mixer_kernel,
        out_shape=(sds((512, 256), F32), sds((512, 256), BF), sds((512, 256), F32), sds((64, 256), BF),
                   t_shape, t_shape),
        in_specs=vspec(4) + [any_spec] * 2,
        out_specs=tuple(vspec(4)) + (any_spec, any_spec),
        scratch_shapes=[
            VMEM((512, 256), BF), VMEM((1024, 256), BF), VMEM((1024, 256), F32), VMEM((64, 256), F32),
            VMEM((512, 256), F32), VMEM((128, 256), BF), VMEM((2, 4, 4, 16, 256), BF),
            dma((16,)), dma((16,)), dma((2,)),
            VMEM((128, 256), BF), VMEM((128, 256), BF), VMEM((4, 128, 256), BF),
            VMEM((128, 256), BF), VMEM((4, 128, 256), BF),
            dma, dma, dma((4,)), dma((4,)), dma((4,)), dma((4,)),
        ],
        compiler_params=pltpu.CompilerParams(collective_id=0, has_side_effects=True),
        cost_estimate=pl.CostEstimate(flops=6_000_000_000, bytes_accessed=6_000_000, transcendentals=0),
        name="mixer_state",
    )(projected, decay_bias_table.T, erase_bias_table.reshape(1, 4), self_token_scale, s0, s1)

    p_shapes = [sds(part_shape(part, 0), BF) for part in PARTS]
    q_shapes = [sds(part_shape(part, 3), BF) for part in PARTS]
    *parts, far, other = pl.pallas_call(
        expert_kernel,
        out_shape=(*p_shapes, sds((128, 2048), BF), sds((3, 128, 2048), BF)),
        in_specs=vspec(2) + [any_spec] * 4,
        out_specs=(*vspec(4), any_spec, any_spec),
        scratch_shapes=[
            VMEM((512, 2048), BF),
            VMEM((4, 2048, 256), BF), VMEM((4, 2048, 256), BF), VMEM((4, 1024, 512), BF),
            VMEM((4, 512, 256), BF),
            dma((4,)), dma((4,)), dma((4,)), dma((2,)), dma((2,)), dma((3,)), dma((3,)),
        ],
        compiler_params=pltpu.CompilerParams(collective_id=2, has_side_effects=True),
        cost_estimate=pl.CostEstimate(flops=8_000_000_000, bytes_accessed=16_000_000, transcendentals=0),
        name="experts",
    )(t0, t1, routed_gate_weight[0], routed_up_weight[0], routed_down_weight[0], near)

    mixer_rows, shared_term, *back = pl.pallas_call(
        finish_kernel,
        out_shape=(sds((128, 2048), BF), sds((128, 2048), F32), *q_shapes),
        in_specs=vspec(6) + [any_spec] * 11,
        out_specs=(*vspec(2), *[any_spec] * 4),
        scratch_shapes=[
            VMEM((512, 256), BF), VMEM((4, 128, 256), BF), VMEM((4, 256, 2048), BF),
            VMEM((2048, 256), BF), VMEM((2048, 256), BF), VMEM((256, 2048), BF),
            *[VMEM(part_shape(part, k), BF) for part in PARTS for k in (1, 2)],
            dma((7,)), dma((3,)), dma((4,)), dma((4,)), dma((4, 3, 8)), dma((4, 3, 8)), dma((4, 3)),
        ],
        compiler_params=pltpu.CompilerParams(collective_id=3, has_side_effects=True),
        cost_estimate=pl.CostEstimate(flops=5_000_000_000, bytes_accessed=6_000_000, transcendentals=0),
        name="mixer_finish",
    )(out_l, rt, selft, enter, head_norm_scale.reshape(1, 256), normed_b, *parts,
      output_weight, near, far, other, common_gate_weight, common_up_weight, common_down_weight)

    mixer_output, mixed_b = pl.pallas_call(
        combine_kernel,
        out_shape=(sds((128, 2048), BF), sds((128, 2048), BF)),
        in_specs=vspec(7),
        out_specs=tuple(vspec(2)),
        scratch_shapes=[VMEM((512, 2048), BF)],
        cost_estimate=pl.CostEstimate(flops=1_000_000_000, bytes_accessed=4_000_000, transcendentals=0),
        name="combine",
    )(*back, weights, shared_term, mixer_rows)
    return (mixer_output, mixed_b)


def solution(mesh):
    split = Mesh(mesh.devices.reshape(4, 4, 2, mesh.shape["tp"]), ("ep_0", "ep_1", "ep_2", "tp"))
    in_specs = (
        P(EP_TP, None), P(), P(EP, "tp"), P("tp"),
        P(None, "tp"), P(None, "tp"), P(None, "tp"), P(None, "tp"), P(None, "tp"),
        P("tp", None), P("tp"), P("tp", None),
        P(EP_TP, None), P(), P(EP_TP, None), P(EP_TP, None),
        P(EP_TP, None, None), P(EP_TP, None, None), P(EP_TP, None, None),
        P(), P(), P(),
    )
    out_specs = (P(EP_TP, None), P(EP_TP, None))
    return jax.shard_map(
        per_device, mesh=split, in_specs=in_specs, out_specs=out_specs, check_vma=False
    )
```
